128 devices in a mesh: ep: 16 (over z, x), tp: 8 (over y, core).
Axes of the slice: x: 4, y: 4, z: 4, core: 2. Of those that a mesh axis runs over, the one named last changes fastest.
Arguments:
- residual: bfloat16 [1024, 4096], P('ep', 'tp'), may hold values from -64 to 64
- routes: int32 [1024, 2], P('ep'), may hold values from 0 to 15, all different within a row; in each aligned block of 64 rows (0 to 63, 64 to 127, ...) at most 16 rows name the same one
- route_weights: float32 [1024, 2], P('ep'), may hold values from 0.2 to 1
- state_prev: float32 [1024, 2, 64, 64], P('ep', None, 'tp'), may hold values from -6 to 6
- mix_gain: float32 [4096], replicated, may hold values from 0.1 to 1.9
- ffn_gain: float32 [4096], replicated, may hold values from 0.1 to 1.9
- w_in: bfloat16 [4096, 1024], P(None, 'tp'), may hold values from -0.09375 to 0.09375
- decay_rate: float32 [64, 64], P('tp'), may hold values from 0.5 to 8
- rotation: float32 [64, 64], P('tp'), may hold values from 0 to 200
- log_step: float32 [64], P('tp'), may hold values from -3.9 to -1.2
- in_re: float32 [64, 64, 16], P('tp'), may hold values from -1 to 1
- in_im: float32 [64, 64, 16], P('tp'), may hold values from -1 to 1
- read_re: float32 [64, 16, 64], P('tp'), may hold values from -0.5 to 0.5
- read_im: float32 [64, 16, 64], P('tp'), may hold values from -0.5 to 0.5
- skip_gain: float32 [64, 16], P('tp'), may hold values from -4 to 4
- w_glu: bfloat16 [1024, 1024], P(None, 'tp'), may hold values from -0.1875 to 0.1875
- w_out: bfloat16 [1024, 4096], P('tp'), may hold values from -0.1875 to 0.1875
- w_gate: bfloat16 [16, 4096, 5632], P('ep', None, 'tp'), may hold values from -0.09375 to 0.09375
- w_up: bfloat16 [16, 4096, 5632], P('ep', None, 'tp'), may hold values from -0.09375 to 0.09375
- w_down: bfloat16 [16, 5632, 4096], P('ep', 'tp'), may hold values from -0.078125 to 0.078125
Outputs:
- layer_out: bfloat16 [1024, 4096], P('ep', 'tp')
- state_next: float32 [1024, 2, 64, 64], P('ep', None, 'tp')
The draws below stay inside these ranges and needn't reach their ends.
Inputs may be any that keep to these rules, and one draw needn't show every extreme that they name: `routes`: each row names 2 different experts. In each aligned block of 64 rows (the rows of one index of ep) no expert is named more than 16 times, a bound that some block reaches.
All inputs are finite; a program needn't handle non-finite values.
Results may differ from the reference program's by a relative error of at most 0.012.
Values may be sent and summed in bfloat16 or wider, within the bound.
A program may use at most 64 MiB of HBM per device.

```python
import math
import jax
import jax.numpy as jnp
import numpy as np
from jax import lax

D = 4096
CHAN = 1024
GROUP_CH = 16
GROUPS = 64
STATE = 64
FF_EXP = 5632
TOPK = 2
SEQ_GRP = 64
SEQS = 1024
EXPERTS = 16
CAP = 16
N_EP = 16
N_TP = 8


def draw_residual(key, part):
    first_key, second_key = jax.random.split(jax.random.fold_in(key, 11))
    column_pos = jnp.arange(D, dtype=jnp.float32) / D
    row_scale = jnp.exp(math.log(10.0) * (jax.random.uniform(second_key, (SEQS, 1), jnp.float32) - 0.5))
    base_values = jnp.clip(jax.random.normal(first_key, (SEQS, D), jnp.float32), -6.0, 6.0)
    column_scale = jnp.exp(math.log(10.0) * (column_pos - 0.5))
    return (base_values * column_scale[None, :] * row_scale).astype(jnp.bfloat16)


def shard_levels(rng, dims, cuts, low, largest):
    def one(dim, shards_of):
        heights = jax.random.uniform(jax.random.fold_in(jax.random.fold_in(rng, 6), dim), (shards_of,), jnp.float32, low / len(cuts), largest / len(cuts))
        return jnp.repeat(jnp.exp(heights), dims[dim] // shards_of).reshape((-1,) + (1,) * (len(dims) - dim - 1))

    factor_of = one(*cuts[0])
    for cut in cuts[1:]:
        factor_of = factor_of * one(*cut)
    return factor_of


def deal_out(own_key, own, number, rows, number_of, top, limit, lean):
    sequence = jax.random.permutation(own_key, number_of)
    packed, usual = portions_of(number_of, rows * top, limit, lean, True), portions_of(number_of, rows * top, limit, lean, False)
    places = jnp.arange(number_of)

    def named(sizes, turn):
        used = int((sizes > 0).sum())
        fixed = max(1, used // 4)
        moved = fixed + (places - fixed + turn * (used - fixed)) % max(1, number_of - fixed)
        return jnp.zeros((number_of,), jnp.int32).at[sequence[jnp.where(places < fixed, places, moved)]].set(jnp.asarray(sizes, jnp.int32))

    sizes = jnp.where(number % 4 == 0, named(packed, number // 4), named(usual, number - number // 4 - 1))
    mixed = jax.random.permutation(jax.random.fold_in(own, 3), number_of)
    giver, taker = mixed[0:number_of // 2 * 2:2], mixed[1:number_of // 2 * 2:2]
    room = jnp.minimum(sizes[giver] - 1, limit - sizes[taker]) // 2
    room = jnp.where((giver == sequence[0]) | (taker == sequence[0]) | (sizes[taker] == 0), 0, jnp.maximum(room, 0))
    moved = jax.random.randint(jax.random.fold_in(own, 4), (number_of // 2,), 0, 1 << 20) % (room + 1)
    sizes = sizes.at[giver].add(-moved).at[taker].add(moved)
    items = jnp.searchsorted(jnp.cumsum(sizes), jnp.arange(rows * top), side="right").astype(jnp.int32)
    listing = items.reshape(top, rows).T
    listing = listing[jax.random.permutation(jax.random.fold_in(own, 1), rows)]
    turn = jax.random.randint(jax.random.fold_in(own, 2), (rows, 1), 0, top)
    return jnp.take_along_axis(listing, (jnp.arange(top)[None, :] + turn) % top, axis=1)


def portions_of(amount, total, reach, lean, full):
    portions = [(1 << 20) // math.isqrt(rank ** lean) + 1 for rank in range(1, amount + 1)]
    largest = reach if full else min(reach, max(-(-total // amount), total * portions[0] // sum(portions)))
    least = 1 if total - largest >= amount - 1 else 0
    holding, surplus = [largest] + [least] * (amount - 1), total - largest - least * (amount - 1)
    while surplus > 0:
        movable = [i for i in range(1, amount) if holding[i] < largest] or [i for i in range(1, amount) if holding[i] < reach]
        mass, left = sum([portions[i] for i in movable]), surplus
        for i in movable:
            addition = min(reach - holding[i], max(1, left * portions[i] // mass), surplus)
            holding[i] = holding[i] + addition
            surplus = surplus - addition
    return np.array(holding)


def noise(rng, dims, deviation, bound, shards=(), held_as=jnp.bfloat16):
    factor_of = shard_levels(rng, dims, shards, -0.22, 0.18) if shards else 1.0
    array = jax.random.normal(rng, dims, jnp.float32) * deviation * factor_of
    return jnp.minimum(jnp.maximum(array, -bound), bound).astype(held_as)


def setup_inputs(seed: int = 0) -> dict:
    keys = jax.random.split(jax.random.key(seed), 21)
    residual = draw_residual(jax.random.fold_in(keys[20], 71), 0)
    routes_keys = jax.random.split(jax.random.fold_in(keys[1], 1), SEQS // SEQ_GRP)
    routes_turns = jax.random.permutation(jax.random.fold_in(keys[1], 3), SEQS // SEQ_GRP)
    routes = jax.vmap(lambda own, number: deal_out(jax.random.fold_in(keys[1], 2), own, number, SEQ_GRP, EXPERTS, TOPK, CAP, 1))(routes_keys, routes_turns).reshape((SEQS, TOPK))
    route_weights = jnp.clip(0.2 + 0.8 * jax.random.uniform(keys[2], (SEQS, TOPK), jnp.float32) ** shard_levels(keys[2], (SEQS, TOPK), ((0, 16),), -0.2, 0.2), 0.2, 1.0)
    state_prev = noise(keys[3], (SEQS, 2, GROUPS, STATE), 1.0, 6.0, ((0, 16), (2, 8)), jnp.float32)
    mix_gain = jnp.clip(1.0 + 0.18 * jax.random.normal(keys[4], (D,), jnp.float32), 0.1, 1.9)
    ffn_gain = jnp.clip(1.0 + 0.18 * jax.random.normal(keys[5], (D,), jnp.float32), 0.1, 1.9)
    w_in = noise(keys[6], (D, CHAN), D ** -0.5, 0.09375, ((1, 8),))
    decay_rate = jnp.clip(jnp.exp(math.log(8.0) - 2.7725887 * jax.random.uniform(keys[7], (GROUPS, STATE), jnp.float32) ** shard_levels(keys[7], (GROUPS, STATE), ((0, 8),), -0.2, 0.2)), 0.5, 8.0)
    rotation = jnp.clip(200.0 * jax.random.uniform(keys[8], (GROUPS, STATE), jnp.float32) ** shard_levels(keys[8], (GROUPS, STATE), ((0, 8),), -0.2, 0.2), 0.0, 200.0)
    log_step = jnp.clip(-3.9 + 2.7 * jax.random.uniform(keys[9], (GROUPS,), jnp.float32) ** shard_levels(keys[9], (GROUPS,), ((0, 8),), -0.2, 0.2), -3.9, -1.2)
    in_re = noise(keys[10], (GROUPS, STATE, GROUP_CH), (2 * GROUP_CH) ** -0.5, 1.0, ((0, 8),), jnp.float32)
    in_im = noise(keys[11], (GROUPS, STATE, GROUP_CH), (2 * GROUP_CH) ** -0.5, 1.0, ((0, 8),), jnp.float32)
    read_re = noise(keys[12], (GROUPS, GROUP_CH, STATE), (2 * STATE) ** -0.5, 0.5, ((0, 8),), jnp.float32)
    read_im = noise(keys[13], (GROUPS, GROUP_CH, STATE), (2 * STATE) ** -0.5, 0.5, ((0, 8),), jnp.float32)
    skip_gain = noise(keys[14], (GROUPS, GROUP_CH), 1.0, 4.0, ((0, 8),), jnp.float32)
    w_glu = noise(keys[15], (CHAN, CHAN), CHAN ** -0.5, 0.1875, ((1, 8),))
    w_out = noise(keys[16], (CHAN, D), CHAN ** -0.5, 0.1875, ((0, 8),))
    w_gate = noise(keys[17], (EXPERTS, D, FF_EXP), D ** -0.5, 0.09375, ((0, 16), (2, 8)))
    w_up = noise(keys[18], (EXPERTS, D, FF_EXP), D ** -0.5, 0.09375, ((0, 16), (2, 8)))
    w_down = noise(keys[19], (EXPERTS, FF_EXP, D), FF_EXP ** -0.5, 0.078125, ((0, 16), (1, 8)))
    return dict(residual=residual, routes=routes, route_weights=route_weights, state_prev=state_prev, mix_gain=mix_gain, ffn_gain=ffn_gain, w_in=w_in, decay_rate=decay_rate, rotation=rotation, log_step=log_step, in_re=in_re, in_im=in_im, read_re=read_re, read_im=read_im, skip_gain=skip_gain, w_glu=w_glu, w_out=w_out, w_gate=w_gate, w_up=w_up, w_down=w_down)


epsilon = 1e-06
highest = lax.Precision.HIGHEST

def inverse_rms(values):
    return lax.rsqrt(lax.optimization_barrier(jnp.mean(values * values, axis=-1, keepdims=True)) + epsilon)

def state_mixer(u_in, state_prev, decay_rate, rotation, log_step, in_re, in_im, read_re, read_im, skip_gain):
    batch_rows = u_in.shape[0]
    groups = decay_rate.shape[0]
    grouped = u_in.astype(jnp.float32).reshape(batch_rows, groups, GROUP_CH)
    step_size = jnp.exp(log_step)[:, None]
    real_part = -decay_rate
    magnitude = jnp.exp(real_part * step_size)
    decay_re = magnitude * jnp.cos(rotation * step_size)
    decay_im = magnitude * jnp.sin(rotation * step_size)
    denominator = real_part * real_part + rotation * rotation
    lift_re = ((decay_re - 1.0) * real_part + decay_im * rotation) / denominator
    lift_im = (decay_im * real_part - (decay_re - 1.0) * rotation) / denominator
    map_re = lift_re[..., None] * in_re - lift_im[..., None] * in_im
    map_im = lift_re[..., None] * in_im + lift_im[..., None] * in_re
    drive_re = jnp.einsum('gph,bgh->bgp', map_re, grouped, precision=highest)
    drive_im = jnp.einsum('gph,bgh->bgp', map_im, grouped, precision=highest)
    old_re = state_prev[:, 0]
    old_im = state_prev[:, 1]
    new_re = decay_re * old_re - decay_im * old_im + drive_re
    new_im = decay_re * old_im + decay_im * old_re + drive_im
    output = jnp.einsum('ghp,bgp->bgh', read_re, new_re, precision=highest) - jnp.einsum('ghp,bgp->bgh', read_im, new_im, precision=highest) + skip_gain * grouped
    return (jax.nn.gelu(output.reshape(batch_rows, -1)), jnp.stack([new_re, new_im], axis=1))

def reference(residual, routes, route_weights, state_prev, mix_gain, ffn_gain, w_in, decay_rate, rotation, log_step, in_re, in_im, read_re, read_im, skip_gain, w_glu, w_out, w_gate, w_up, w_down):
    source = residual.astype(jnp.float32)
    normed_mix = (source * inverse_rms(source) * mix_gain).astype(jnp.bfloat16)
    u_in = jnp.dot(normed_mix, w_in, preferred_element_type=jnp.float32).astype(jnp.bfloat16)
    mixer_act, state_next = state_mixer(u_in, state_prev, decay_rate, rotation, log_step, in_re, in_im, read_re, read_im, skip_gain)
    mixer_bf = mixer_act.astype(jnp.bfloat16)
    glu_logit = jnp.dot(mixer_bf, w_glu, preferred_element_type=jnp.float32)
    mixed = (mixer_act * jax.nn.sigmoid(glu_logit)).astype(jnp.bfloat16)
    block_width = CHAN // N_TP
    branch = jnp.zeros((SEQS, D), jnp.float32)
    for shard in range(N_TP):
        partial_block = jnp.dot(mixed[:, shard * block_width:(shard + 1) * block_width], w_out[shard * block_width:(shard + 1) * block_width], preferred_element_type=jnp.float32).astype(jnp.bfloat16)
        branch = branch + lax.optimization_barrier(partial_block).astype(jnp.float32)
    after_mix = (source + branch).astype(jnp.bfloat16)
    after_float = after_mix.astype(jnp.float32)
    normed_ffn = (after_float * inverse_rms(after_float) * ffn_gain).astype(jnp.bfloat16)
    expert_ids = jnp.arange(EXPERTS, dtype=jnp.int32)
    onehot = (routes[:, :, None] == expert_ids).astype(jnp.int32)
    blocked = onehot.reshape(N_EP, SEQ_GRP * TOPK, EXPERTS)
    before = jnp.cumsum(blocked, axis=1) - blocked
    slot_index = lax.optimization_barrier(jnp.sum(before * blocked, axis=-1)).reshape(SEQS, TOPK)
    group_of_row = jnp.arange(SEQS, dtype=jnp.int32) // SEQ_GRP
    position = group_of_row[:, None] * CAP + slot_index
    columns = jnp.arange(N_EP * CAP, dtype=jnp.int32)
    hidden_width = FF_EXP // N_TP
    normed_float = normed_ffn.astype(jnp.float32)

    def apply_expert(running, expert):
        matches = (routes == expert)[:, :, None] & (position[:, :, None] == columns)
        select = jnp.any(matches, axis=1).astype(jnp.float32)
        weighting = lax.optimization_barrier(jnp.sum(jnp.where(matches, route_weights[:, :, None], 0.0), axis=1))
        expert_in = jnp.dot(select.T, normed_float, precision=highest).astype(jnp.bfloat16)
        gate_value = jnp.dot(expert_in, w_gate[expert], preferred_element_type=jnp.float32)
        up_value = jnp.dot(expert_in, w_up[expert], preferred_element_type=jnp.float32)
        hidden = (jax.nn.silu(gate_value) * up_value).astype(jnp.bfloat16)
        down_weight = w_down[expert]
        summed = jnp.zeros((N_EP * CAP, D), jnp.float32)
        for shard in range(N_TP):
            partial_block = jnp.dot(hidden[:, shard * hidden_width:(shard + 1) * hidden_width], down_weight[shard * hidden_width:(shard + 1) * hidden_width], preferred_element_type=jnp.float32).astype(jnp.bfloat16)
            summed = summed + lax.optimization_barrier(partial_block).astype(jnp.float32)
        expert_out = summed.astype(jnp.bfloat16)
        added = jnp.dot(weighting, expert_out.astype(jnp.float32), precision=highest)
        return (running + added, None)
    combined, _ = lax.scan(apply_expert, jnp.zeros((SEQS, D), jnp.float32), expert_ids)
    layer_out = (after_float + combined).astype(jnp.bfloat16)
    return (layer_out, state_next)
```

```python
import functools

import jax
import jax.numpy as jnp
from jax import lax
from jax.experimental import pallas as pl
from jax.experimental.pallas import tpu as pltpu
from jax.sharding import PartitionSpec as P

MESH = pl.DeviceIdType.MESH
BF = jnp.bfloat16
F32 = jnp.float32
EPS = 1e-06
NT = (((1,), (1,)), ((), ()))

NEP = 16
NTP = 8
ROWS = 64
WIDTH = 512
SLOT = 16
SLOTS = NEP * SLOT
FFW = 704
STATE = 64
GRP = 8
GCH = 16


def dot(a, b):
    return jnp.dot(a, b, preferred_element_type=F32)


def dot_nt(a, b):
    return lax.dot_general(a, b, NT, preferred_element_type=F32)


def iota(shape, dim):
    return lax.broadcasted_iota(jnp.int32, shape, dim)


def kernel(
    residual, routes, weights, state, mix_gain, ffn_gain, w_in, decay_rate, rotation,
    log_step, in_re, in_im, read_re, read_im, skip, w_glu, w_out, w_gate, w_up, w_down,
    out, state_out,
    v_routes, v_weights, v_state, v_mix, v_ffn, v_win, v_rate, v_rot, v_step, v_inre,
    v_inim, v_rre, v_rim, v_skip, v_glu, v_out, v_gate, v_up, v_down,
    g1, bd_hi, bd_lo, rbd, fresh, new_state, act_all, act32, mixed,
    b_ds, b_dr, b_q, b_own, b_rel, b_dir, b_mrg, b_ms,
    after, d_map, wt, outb, g2, acc_g, acc_u, sq, hidden,
    e_ds, e_dr, e_q, e_own, e_rel, e_dir, e_mrg, e_ms, eout, back, v_layer,
    load_sem, g1_s, g1_r, a_s, a_r, b_s, b_r, x_s, x_r, g2_s, g2_r, e_s, e_r, ret_s, ret_r, st_sem,
):
    ep = lax.axis_index("ep")
    tp = lax.axis_index("tp")
    y, c = lax.div(tp, 2), lax.rem(tp, 2)
    z, x = lax.div(ep, 4), lax.rem(ep, 4)
    yp, ym, yo = lax.rem(y + 1, 4), lax.rem(y + 3, 4), lax.rem(y + 2, 4)
    oc = 1 - c
    partner = y * 2 + oc
    up, down = yp * 2 + c, ym * 2 + c
    sent = []

    def send(src, dst, ss, rs, device):
        copy = pltpu.make_async_remote_copy(
            src_ref=src, dst_ref=dst, send_sem=ss, recv_sem=rs, device_id=device, device_id_type=MESH
        )
        copy.start()
        sent.append(copy)

    def arrive(dst, ss, rs):
        pltpu.make_async_remote_copy(
            src_ref=dst, dst_ref=dst, send_sem=ss, recv_sem=rs, device_id=(ep, partner), device_id_type=MESH
        ).wait_recv()

    pairs = [
        (residual, g1.at[tp]), (w_in, v_win), (mix_gain, v_mix),
        (decay_rate, v_rate), (rotation, v_rot), (log_step, v_step), (in_re, v_inre), (in_im, v_inim),
        (read_re, v_rre), (read_im, v_rim), (skip, v_skip), (routes, v_routes), (weights, v_weights),
        (state, v_state), (w_glu, v_glu), (w_out, v_out), (ffn_gain, v_ffn),
        (w_gate, v_gate), (w_up, v_up), (w_down, v_down),
    ]
    loads = [pltpu.make_async_copy(src, dst, load_sem.at[i]) for i, (src, dst) in enumerate(pairs)]
    for load in loads:
        load.start()

    barrier = pltpu.get_barrier_semaphore()
    for d in range(1, NTP):
        pl.semaphore_signal(barrier, inc=1, device_id=(ep, lax.rem(tp + d, NTP)), device_id_type=MESH)
    for d in range(1, NEP):
        pl.semaphore_signal(barrier, inc=1, device_id=(lax.rem(ep + d, NEP), tp), device_id_type=MESH)

    for i in range(3, 14):
        loads[i].wait()

    eye8 = iota((GRP, GRP), 0) == iota((GRP, GRP), 1)
    step = jnp.exp(jnp.sum(jnp.where(eye8, jnp.broadcast_to(v_step[...], (GRP, GRP)), 0.0), axis=1, keepdims=True))
    rate, rot = v_rate[...], v_rot[...]
    real = -rate
    magnitude = jnp.exp(real * step)
    angle = rot * step
    decay_re = magnitude * jnp.cos(angle)
    decay_im = magnitude * jnp.sin(angle)
    denominator = real * real + rot * rot
    lift_re = ((decay_re - 1.0) * real + decay_im * rot) / denominator
    lift_im = (decay_im * real - (decay_re - 1.0) * rot) / denominator
    bd_hi[...] = jnp.zeros_like(bd_hi)
    bd_lo[...] = jnp.zeros_like(bd_lo)
    rbd[...] = jnp.zeros_like(rbd)
    fresh[...] = jnp.zeros_like(fresh)
    for g in range(GRP):
        rows = slice(g * GCH, (g + 1) * GCH)
        l_re, l_im = lift_re[g:g + 1, :], lift_im[g:g + 1, :]
        b_re, b_im = v_inre[rows, :], v_inim[rows, :]
        for n, value in enumerate((l_re * b_re - l_im * b_im, l_re * b_im + l_im * b_re)):
            lanes = slice((2 * g + n) * 128, (2 * g + n) * 128 + STATE)
            hi = value.astype(BF)
            bd_hi[rows, lanes] = hi
            bd_lo[rows, lanes] = (value - hi.astype(F32)).astype(BF)
        rbd[rows, (2 * g) * 128:(2 * g) * 128 + STATE] = v_rre[rows, :].astype(BF)
        rbd[rows, (2 * g + 1) * 128:(2 * g + 1) * 128 + STATE] = (-v_rim[rows, :]).astype(BF)
    tiler = (iota((GCH, 128), 0) == lax.rem(iota((GCH, 128), 1), GCH)).astype(BF)
    skip_hi = v_skip[...].astype(BF)
    skip_rest = v_skip[...] - skip_hi.astype(F32)
    skip_mid = skip_rest.astype(BF)
    skip_lo = (skip_rest - skip_mid.astype(F32)).astype(BF)
    skip_rep = dot(skip_hi, tiler) + dot(skip_mid, tiler) + dot(skip_lo, tiler)
    skip_row = jnp.sum(
        jnp.where(lax.div(iota((GRP, 128), 1), GCH) == iota((GRP, 128), 0), skip_rep, 0.0), axis=0, keepdims=True
    )
    r0, r1 = v_routes[0:1, :], v_routes[1:2, :]
    oh0 = (r0 == iota((NEP, ROWS), 0)).astype(F32)
    oh1 = (r1 == iota((NEP, ROWS), 0)).astype(F32)
    upper_tri = (iota((ROWS, ROWS), 0) < iota((ROWS, ROWS), 1)).astype(BF)
    before = dot((oh0 + oh1).astype(BF), upper_tri)
    dest0 = r0.astype(F32) * SLOT + jnp.sum(before * oh0, axis=0, keepdims=True)
    dest1 = r1.astype(F32) * SLOT + jnp.sum(before * oh1, axis=0, keepdims=True)
    place = iota((SLOTS, ROWS), 0).astype(F32)
    m0, m1 = (dest0 == place).astype(F32), (dest1 == place).astype(F32)
    d_map[...] = (m0 + m1).astype(BF)
    w_all = jnp.transpose(v_weights[0:1, :] * m0 + v_weights[1:2, :] * m1)
    w_hi = w_all.astype(BF)
    wt[0] = w_hi
    wt[1] = (w_all - w_hi.astype(F32)).astype(BF)

    def gather_send(buf, half, ss, rs, rows):
        send(buf(tp, *rows), buf(tp, *rows), ss(0), rs(0), (ep, up))
        send(buf(tp, *rows), buf(tp, *rows), ss(1), rs(1), (ep, down))
        send(buf(tp, *rows), buf(tp, *rows), ss(4), rs(4), (ep, partner))

    def gather_relay(buf, half, ss, rs, rows):
        first, size = rows
        lo_half, hi_half = (first, half), (first + half, half)
        arrive(buf(down, *rows), ss(0), rs(0))
        send(buf(down, *lo_half), buf(down, *lo_half), ss(2), rs(2), (ep, up))
        send(buf(down, *rows), buf(down, *rows), ss(5), rs(5), (ep, partner))
        arrive(buf(up, *rows), ss(1), rs(1))
        send(buf(up, *hi_half), buf(up, *hi_half), ss(3), rs(3), (ep, down))
        send(buf(up, *rows), buf(up, *rows), ss(6), rs(6), (ep, partner))

    far, far_oc = yo * 2 + c, yo * 2 + oc
    up_oc, down_oc = yp * 2 + oc, ym * 2 + oc

    def gather_far(buf, half, ss, rs, rows):
        first, size = rows
        lo_half, hi_half = (first, half), (first + half, half)
        arrive(buf(far, *lo_half), ss(2), rs(2))
        send(buf(far, *lo_half), buf(far, *lo_half), ss(7), rs(7), (ep, partner))
        arrive(buf(far, *hi_half), ss(3), rs(3))
        send(buf(far, *hi_half), buf(far, *hi_half), ss(8), rs(8), (ep, partner))

    def at1(t, first, size):
        return g1.at[t, pl.ds(first, size), :]

    one = (at1, ROWS // 2, lambda k: g1_s.at[k], lambda k: g1_r.at[k], (0, ROWS))
    loads[0].wait()
    pl.semaphore_wait(barrier, NTP + NEP - 2)
    gather_send(*one)
    loads[1].wait()
    loads[2].wait()

    total = [None, None]

    def mix_block(t):
        rows = g1[t].astype(F32)
        squares = jnp.sum(rows * rows, axis=1, keepdims=True)
        gain = v_mix[:, pl.ds(pl.multiple_of(t * WIDTH, WIDTH), WIDTH)]
        product = dot((rows * gain).astype(BF), v_win[pl.ds(pl.multiple_of(t * WIDTH, WIDTH), WIDTH), :])
        total[0] = squares if total[0] is None else total[0] + squares
        total[1] = product if total[1] is None else total[1] + product

    mix_block(tp)
    gather_relay(*one)
    mix_block(down)
    mix_block(up)
    arrive(at1(partner, 0, ROWS), g1_s.at[4], g1_r.at[4])
    mix_block(partner)
    gather_far(*one)
    arrive(at1(down_oc, 0, ROWS), g1_s.at[5], g1_r.at[5])
    mix_block(down_oc)
    arrive(at1(up_oc, 0, ROWS), g1_s.at[6], g1_r.at[6])
    mix_block(up_oc)
    mix_block(far)
    arrive(at1(far_oc, 0, ROWS // 2), g1_s.at[7], g1_r.at[7])
    arrive(at1(far_oc, ROWS // 2, ROWS // 2), g1_s.at[8], g1_r.at[8])
    mix_block(far_oc)
    u_in = (total[1] * lax.rsqrt(total[0] / (NTP * WIDTH) + EPS)).astype(BF)

    drive = dot(u_in, bd_hi[...]) + dot(u_in, bd_lo[...])
    for g in range(GRP):
        old_re = v_state[pl.ds(g, ROWS, stride=2 * GRP), :]
        old_im = v_state[pl.ds(GRP + g, ROWS, stride=2 * GRP), :]
        k_re, k_im = decay_re[g:g + 1, :], decay_im[g:g + 1, :]
        new_re = k_re * old_re - k_im * old_im + drive[:, (2 * g) * 128:(2 * g) * 128 + STATE]
        new_im = k_re * old_im + k_im * old_re + drive[:, (2 * g + 1) * 128:(2 * g + 1) * 128 + STATE]
        new_state[pl.ds(g, ROWS, stride=2 * GRP), :] = new_re
        new_state[pl.ds(GRP + g, ROWS, stride=2 * GRP), :] = new_im
        fresh[:, (2 * g) * 128:(2 * g) * 128 + STATE] = new_re.astype(BF)
        fresh[:, (2 * g + 1) * 128:(2 * g + 1) * 128 + STATE] = new_im.astype(BF)
    act = jax.nn.gelu(dot_nt(fresh[...], rbd[...]) + skip_row * u_in.astype(F32))
    act32[...] = act
    act_all[tp] = act.astype(BF)
    for d in range(1, NTP):
        send(act_all.at[tp], act_all.at[tp], a_s.at[d], a_r.at[d], (ep, lax.rem(tp + d, NTP)))
    store_state = pltpu.make_async_copy(new_state, state_out, st_sem)
    store_state.start()
    loads[14].wait()
    loads[15].wait()
    for d in range(1, NTP):
        arrive(act_all.at[lax.rem(tp + NTP - d, NTP)], a_s.at[d], a_r.at[d])
    logit = dot(jnp.concatenate([act_all[t] for t in range(NTP)], axis=1), v_glu[...])
    mixed[...] = (act32[...] * jax.nn.sigmoid(logit)).astype(BF)

    order = (yo, yp, ym, y)

    def reduce_scatter(product, rows, sets, ds, dr, q, own, rel, dire, mrg, ms, ss, rs, done):
        half = rows // 2
        piece = half // sets
        base = 4

        def lo(i):
            return pl.ds(i * piece, piece)

        def hi(i):
            return pl.ds(half + i * piece, piece)

        def sem(kind, i):
            return base + kind * sets + i

        for j in range(4):
            ds[j] = product(order[j] * 2 + oc).astype(BF)
            send(ds.at[j], dr.at[j], ss.at[j], rs.at[j], (ep, partner))

        def on_chip(j):
            value = product(order[j] * 2 + c)
            arrive(dr.at[j], ss.at[j], rs.at[j])
            return value + dr[j].astype(F32)

        q[0] = on_chip(0).astype(BF)
        for i in range(sets):
            send(q.at[0, lo(i), :], rel.at[0, lo(i), :], ss.at[sem(0, i)], rs.at[sem(0, i)], (ep, up))
            send(q.at[0, hi(i), :], rel.at[1, lo(i), :], ss.at[sem(1, i)], rs.at[sem(1, i)], (ep, down))
        q[1] = on_chip(1).astype(BF)

        def direct_up(i):
            send(q.at[1, hi(i), :], dire.at[0, lo(i), :], ss.at[sem(2, i)], rs.at[sem(2, i)], (ep, up))

        def direct_down(i):
            send(q.at[2, lo(i), :], dire.at[1, lo(i), :], ss.at[sem(3, i)], rs.at[sem(3, i)], (ep, down))

        direct_up(0)
        q[2] = on_chip(2).astype(BF)
        direct_down(0)
        own[...] = on_chip(3)
        for i in range(sets):
            if i:
                direct_up(i)
                direct_down(i)
            arrive(rel.at[0, lo(i), :], ss.at[sem(0, i)], rs.at[sem(0, i)])
            ms[0, i * piece:(i + 1) * piece, :] = (
                q[1, i * piece:(i + 1) * piece, :].astype(F32) + rel[0, i * piece:(i + 1) * piece, :].astype(F32)
            ).astype(BF)
            send(ms.at[0, lo(i), :], mrg.at[0, lo(i), :], ss.at[sem(4, i)], rs.at[sem(4, i)], (ep, up))
            arrive(rel.at[1, lo(i), :], ss.at[sem(1, i)], rs.at[sem(1, i)])
            ms[1, i * piece:(i + 1) * piece, :] = (
                q[2, half + i * piece:half + (i + 1) * piece, :].astype(F32)
                + rel[1, i * piece:(i + 1) * piece, :].astype(F32)
            ).astype(BF)
            send(ms.at[1, lo(i), :], mrg.at[1, lo(i), :], ss.at[sem(5, i)], rs.at[sem(5, i)], (ep, down))
        for i in range(sets):
            part = slice(i * piece, (i + 1) * piece)
            arrive(dire.at[1, lo(i), :], ss.at[sem(3, i)], rs.at[sem(3, i)])
            arrive(mrg.at[0, lo(i), :], ss.at[sem(4, i)], rs.at[sem(4, i)])
            done(i * piece, piece, own[part, :] + dire[1, part, :].astype(F32) + mrg[0, part, :].astype(F32))
            top = slice(half + i * piece, half + (i + 1) * piece)
            arrive(dire.at[0, lo(i), :], ss.at[sem(2, i)], rs.at[sem(2, i)])
            arrive(mrg.at[1, lo(i), :], ss.at[sem(5, i)], rs.at[sem(5, i)])
            done(half + i * piece, piece, own[top, :] + dire[0, part, :].astype(F32) + mrg[1, part, :].astype(F32))

    def columns(t):
        return pl.ds(pl.multiple_of(t * WIDTH, WIDTH), WIDTH)

    def branch_done(first, size, value):
        source = g1[tp, first:first + size, :].astype(F32)
        after[first:first + size, :] = (source + value).astype(BF)

    reduce_scatter(
        lambda t: dot(mixed[...], v_out[:, columns(t)]), ROWS, 1,
        b_ds, b_dr, b_q, b_own, b_rel, b_dir, b_mrg, b_ms, b_s, b_r, branch_done,
    )

    outb[...] = dot(d_map[...], after[...]).astype(BF)

    def slot(e):
        return pl.ds(pl.multiple_of(e * SLOT, SLOT), SLOT)

    hops = [(dz, dx) for dz in (0, 1, 3, 2) for dx in (1, 3, 2, 0) if (dz, dx) != (0, 0)]
    for dz, dx in hops:
        k = dz * 4 + dx
        e = lax.rem(z + dz, 4) * 4 + lax.rem(x + dx, 4)
        send(outb.at[slot(e), :], g2.at[tp, slot(ep), :], x_s.at[k], x_r.at[k], (e, tp))
    g2[tp, slot(ep), :] = outb[slot(ep), :]
    loads[16].wait()
    loads[17].wait()
    loads[18].wait()

    def at2(t, first, size):
        return g2.at[t, pl.ds(first, size), :]

    def sems2(table, j):
        return lambda k: table.at[j, k]

    chunk = SLOTS // 4
    turns = (0, 1, 3, 2)
    plans = []
    for j, dz in enumerate(turns):
        first = pl.multiple_of(lax.rem(z + 4 - dz, 4) * chunk, chunk)
        plans.append((at2, chunk // 2, sems2(g2_s, j), sems2(g2_r, j), (first, chunk)))

    def start_chunk(j):
        dz = turns[j]
        for dx in (1, 3, 2, 0):
            if (dz, dx) == (0, 0):
                continue
            k = dz * 4 + dx
            s = lax.rem(z + 4 - dz, 4) * 4 + lax.rem(x + 4 - dx, 4)
            arrive(g2.at[tp, slot(s), :], x_s.at[k], x_r.at[k])
        gather_send(*plans[j])

    began = []

    def expert_block(t):
        gain = v_ffn[:, columns(t)]
        rows = g2[t].astype(F32)
        scaled = (rows * gain).astype(BF)
        squares = rows * rows
        squares = squares[:, 0:128] + squares[:, 128:256] + squares[:, 256:384] + squares[:, 384:512]
        gate, upper = dot_nt(scaled, v_gate[:, columns(t)]), dot_nt(scaled, v_up[:, columns(t)])
        if began:
            sq[...] += squares
            acc_g[...] += gate
            acc_u[...] += upper
        else:
            began.append(True)
            sq[...] = squares
            acc_g[...] = gate
            acc_u[...] = upper

    def from_partner(t, kinds):
        for j in range(4):
            at, half, ss, rs, (first, size) = plans[j]
            if len(kinds) == 1:
                arrive(at(t, first, size), ss(kinds[0]), rs(kinds[0]))
            else:
                arrive(at(t, first, half), ss(kinds[0]), rs(kinds[0]))
                arrive(at(t, first + half, half), ss(kinds[1]), rs(kinds[1]))

    start_chunk(0)
    start_chunk(1)
    gather_relay(*plans[0])
    start_chunk(2)
    gather_relay(*plans[1])
    gather_far(*plans[0])
    start_chunk(3)
    gather_relay(*plans[2])
    gather_far(*plans[1])
    expert_block(tp)
    gather_relay(*plans[3])
    from_partner(partner, (4,))
    expert_block(partner)
    gather_far(*plans[2])
    expert_block(down)
    expert_block(up)
    gather_far(*plans[3])
    from_partner(down_oc, (5,))
    expert_block(down_oc)
    from_partner(up_oc, (6,))
    expert_block(up_oc)
    expert_block(far)
    from_partner(far_oc, (7, 8))
    expert_block(far_oc)

    loads[19].wait()
    for r in range(0, SLOTS, 64):
        scale = lax.rsqrt(jnp.sum(sq[r:r + 64, :], axis=1, keepdims=True) / (NTP * WIDTH) + EPS)
        gate, upper = acc_g[r:r + 64, :] * scale, acc_u[r:r + 64, :] * scale
        hidden[r:r + 64, :] = (gate * jax.nn.sigmoid(gate) * upper).astype(BF)

    def expert_done(first, size, value):
        eout[first:first + size, :] = value.astype(BF)
        for s in range(first // SLOT, (first + size) // SLOT):
            rows = slice(s * SLOT, (s + 1) * SLOT)

            @pl.when(ep == s)
            def _():
                back[rows, :] = eout[rows, :]

            @pl.when(ep != s)
            def _():
                pltpu.make_async_remote_copy(
                    src_ref=eout.at[pl.ds(s * SLOT, SLOT), :], dst_ref=back.at[slot(ep), :],
                    send_sem=ret_s.at[s], recv_sem=ret_r.at[ep], device_id=(s, tp), device_id_type=MESH,
                ).start()

    reduce_scatter(
        lambda t: dot(hidden[...], v_down[:, columns(t)]), SLOTS, 2,
        e_ds, e_dr, e_q, e_own, e_rel, e_dir, e_mrg, e_ms, e_s, e_r, expert_done,
    )
    for d in range(1, NEP):
        e = lax.rem(ep + d, NEP)
        arrive(back.at[slot(e), :], ret_s.at[e], ret_r.at[e])
    combined = dot(wt[0], back[...]) + dot(wt[1], back[...])
    v_layer[...] = (after[...].astype(F32) + combined).astype(BF)
    finish = pltpu.make_async_copy(v_layer, out, load_sem.at[0])
    finish.start()
    for copy in sent:
        copy.wait_send()
    for d in range(1, NEP):
        e = lax.rem(ep + d, NEP)
        pltpu.make_async_remote_copy(
            src_ref=eout.at[slot(e), :], dst_ref=eout.at[slot(e), :], send_sem=ret_s.at[e], recv_sem=ret_r.at[e],
            device_id=(e, tp), device_id_type=MESH,
        ).wait_send()
    store_state.wait()
    finish.wait()


def per_device(
    residual, routes, route_weights, state_prev, mix_gain, ffn_gain, w_in, decay_rate, rotation,
    log_step, in_re, in_im, read_re, read_im, skip_gain, w_glu, w_out, w_gate, w_up, w_down,
):
    dma = pltpu.SemaphoreType.DMA
    vm = pltpu.VMEM
    operands = (
        residual, routes.T, route_weights.T, state_prev.reshape(ROWS * 2 * GRP, STATE), mix_gain.reshape(1, -1),
        ffn_gain.reshape(1, -1), w_in, decay_rate, rotation, log_step.reshape(1, GRP),
        in_re.transpose(0, 2, 1).reshape(GRP * GCH, STATE), in_im.transpose(0, 2, 1).reshape(GRP * GCH, STATE), read_re.reshape(GRP * GCH, STATE),
        read_im.reshape(GRP * GCH, STATE), skip_gain, w_glu, w_out, w_gate[0].T, w_up[0].T, w_down[0],
    )

    def exchange(rows):
        half = rows // 2
        return [
            vm((4, rows, WIDTH), BF), vm((4, rows, WIDTH), BF), vm((3, rows, WIDTH), BF), vm((rows, WIDTH), F32),
            vm((2, half, WIDTH), BF), vm((2, half, WIDTH), BF), vm((2, half, WIDTH), BF), vm((2, half, WIDTH), BF),
        ]

    scratch = [vm(operands[i].shape, operands[i].dtype) for i in range(1, 20)]
    scratch += [
        vm((NTP, ROWS, WIDTH), BF), vm((128, 2048), BF), vm((128, 2048), BF),
        vm((128, 2048), BF), vm((ROWS, 2048), BF), vm((ROWS * 2 * GRP, STATE), F32), vm((NTP, ROWS, 128), BF),
        vm((ROWS, 128), F32), vm((ROWS, 128), BF),
    ]
    scratch += exchange(ROWS)
    scratch += [
        vm((ROWS, WIDTH), BF), vm((SLOTS, ROWS), BF), vm((2, ROWS, SLOTS), BF), vm((SLOTS, WIDTH), BF),
        vm((NTP, SLOTS, WIDTH), BF), vm((SLOTS, FFW), F32), vm((SLOTS, FFW), F32), vm((SLOTS, 128), F32),
        vm((SLOTS, FFW), BF),
    ]
    scratch += exchange(SLOTS)
    scratch += [vm((SLOTS, WIDTH), BF), vm((SLOTS, WIDTH), BF), vm((ROWS, WIDTH), BF)]
    scratch += [
        dma((20,)), dma((9,)), dma((9,)), dma((8,)), dma((8,)), dma((10,)), dma((10,)), dma((16,)), dma((16,)),
        dma((4, 9)), dma((4, 9)), dma((16,)), dma((16,)), dma((16,)), dma((16,)), dma,
    ]
    anywhere = pl.BlockSpec(memory_space=pl.ANY)
    layer_out, state_next = pl.pallas_call(
        kernel,
        out_shape=(
            jax.ShapeDtypeStruct((ROWS, WIDTH), BF),
            jax.ShapeDtypeStruct((ROWS * 2 * GRP, STATE), F32),
        ),
        in_specs=[anywhere] * 20,
        out_specs=(anywhere, anywhere),
        scratch_shapes=scratch,
        compiler_params=pltpu.CompilerParams(
            collective_id=0, has_side_effects=True, vmem_limit_bytes=60 * 1024 * 1024
        ),
        name="layer",
    )(*operands)
    return layer_out, state_next.reshape(ROWS, 2, GRP, STATE)


def solution(mesh):
    return jax.shard_map(
        per_device,
        mesh=mesh,
        in_specs=(
            P("ep", "tp"), P("ep", None), P("ep", None), P("ep", None, "tp", None), P(), P(), P(None, "tp"),
            P("tp", None), P("tp", None), P("tp"), P("tp", None, None), P("tp", None, None), P("tp", None, None),
            P("tp", None, None), P("tp", None), P(None, "tp"), P("tp", None), P("ep", None, "tp"),
            P("ep", None, "tp"), P("ep", "tp", None),
        ),
        out_specs=(P("ep", "tp"), P("ep", None, "tp", None)),
        check_vma=False,
    )
```

```python
import functools

import jax
import jax.numpy as jnp
from jax import lax
from jax.experimental import pallas as pl
from jax.experimental.pallas import tpu as pltpu
from jax.sharding import PartitionSpec as P

MESH = pl.DeviceIdType.MESH
BF = jnp.bfloat16
F32 = jnp.float32
EPS = 1e-06
NT = (((1,), (1,)), ((), ()))

NEP = 16
NTP = 8
ROWS = 64
WIDTH = 512
SLOT = 16
SLOTS = NEP * SLOT
FFW = 704
STATE = 64
GRP = 8
GCH = 16


def dot(a, b):
    return jnp.dot(a, b, preferred_element_type=F32)


def dot_nt(a, b):
    return lax.dot_general(a, b, NT, preferred_element_type=F32)


def iota(shape, dim):
    return lax.broadcasted_iota(jnp.int32, shape, dim)


def kernel(
    residual, routes, weights, state, mix_gain, ffn_gain, w_in, decay_rate, rotation,
    log_step, in_re, in_im, read_re, read_im, skip, w_glu, w_out, w_gate, w_up, w_down,
    out, state_out,
    v_routes, v_weights, v_state, v_mix, v_ffn, v_win, v_rate, v_rot, v_step, v_inre,
    v_inim, v_rre, v_rim, v_skip, v_glu, v_out, v_gate, v_up, v_down,
    g1, bd_hi, bd_lo, rbd, fresh, act_all, act32, mixed,
    b_ds, b_dr, b_q, b_own, b_rel, b_dir, b_mrg, b_ms,
    after, d_map, wt, outb, g2, acc_g, acc_u, sq, hidden,
    e_ds, e_dr, e_q, e_own, e_rel, e_dir, e_mrg, e_ms, eout, back,
    load_sem, g1_s, g1_r, a_s, a_r, b_s, b_r, x_s, x_r, g2_s, g2_r, e_s, e_r, ret_s, ret_r,
):
    ep = lax.axis_index("ep")
    tp = lax.axis_index("tp")
    y, c = lax.div(tp, 2), lax.rem(tp, 2)
    z, x = lax.div(ep, 4), lax.rem(ep, 4)
    yp, ym, yo = lax.rem(y + 1, 4), lax.rem(y + 3, 4), lax.rem(y + 2, 4)
    oc = 1 - c
    partner = y * 2 + oc
    up, down = yp * 2 + c, ym * 2 + c
    sent = []

    def send(src, dst, ss, rs, device):
        copy = pltpu.make_async_remote_copy(
            src_ref=src, dst_ref=dst, send_sem=ss, recv_sem=rs, device_id=device, device_id_type=MESH
        )
        copy.start()
        sent.append(copy)

    def arrive(dst, ss, rs):
        pltpu.make_async_remote_copy(
            src_ref=dst, dst_ref=dst, send_sem=ss, recv_sem=rs, device_id=(ep, partner), device_id_type=MESH
        ).wait_recv()

    pairs = [
        (residual, g1.at[tp]), (w_in, v_win), (mix_gain, v_mix),
        (decay_rate, v_rate), (rotation, v_rot), (log_step, v_step), (in_re, v_inre), (in_im, v_inim),
        (read_re, v_rre), (read_im, v_rim), (skip, v_skip), (routes, v_routes), (weights, v_weights),
        (state, v_state), (w_glu, v_glu), (w_out, v_out), (ffn_gain, v_ffn),
        (w_gate, v_gate), (w_up, v_up), (w_down, v_down),
    ]
    loads = [pltpu.make_async_copy(src, dst, load_sem.at[i]) for i, (src, dst) in enumerate(pairs)]
    loads[0].start()

    barrier = pltpu.get_barrier_semaphore()
    for d in range(1, NTP):
        pl.semaphore_signal(barrier, inc=1, device_id=(ep, lax.rem(tp + d, NTP)), device_id_type=MESH)
    for d in range(1, NEP):
        pl.semaphore_signal(barrier, inc=1, device_id=(lax.rem(ep + d, NEP), tp), device_id_type=MESH)

    for load in loads[1:]:
        load.start()

    def gather_send(buf, half, ss, rs, rows):
        send(buf(tp, *rows), buf(tp, *rows), ss(0), rs(0), (ep, up))
        send(buf(tp, *rows), buf(tp, *rows), ss(1), rs(1), (ep, down))
        send(buf(tp, *rows), buf(tp, *rows), ss(4), rs(4), (ep, partner))

    def gather_relay(buf, half, ss, rs, rows):
        first, size = rows
        lo_half, hi_half = (first, half), (first + half, half)
        arrive(buf(down, *rows), ss(0), rs(0))
        send(buf(down, *lo_half), buf(down, *lo_half), ss(2), rs(2), (ep, up))
        send(buf(down, *rows), buf(down, *rows), ss(5), rs(5), (ep, partner))
        arrive(buf(up, *rows), ss(1), rs(1))
        send(buf(up, *hi_half), buf(up, *hi_half), ss(3), rs(3), (ep, down))
        send(buf(up, *rows), buf(up, *rows), ss(6), rs(6), (ep, partner))

    far, far_oc = yo * 2 + c, yo * 2 + oc
    up_oc, down_oc = yp * 2 + oc, ym * 2 + oc

    def gather_far(buf, half, ss, rs, rows):
        first, size = rows
        lo_half, hi_half = (first, half), (first + half, half)
        arrive(buf(far, *lo_half), ss(2), rs(2))
        send(buf(far, *lo_half), buf(far, *lo_half), ss(7), rs(7), (ep, partner))
        arrive(buf(far, *hi_half), ss(3), rs(3))
        send(buf(far, *hi_half), buf(far, *hi_half), ss(8), rs(8), (ep, partner))

    def at1(t, first, size):
        return g1.at[t, pl.ds(first, size), :]

    one = (at1, ROWS // 2, lambda k: g1_s.at[k], lambda k: g1_r.at[k], (0, ROWS))
    loads[0].wait()
    pl.semaphore_wait(barrier, NTP + NEP - 2)
    gather_send(*one)
    for i in range(3, 14):
        loads[i].wait()

    eye8 = iota((GRP, GRP), 0) == iota((GRP, GRP), 1)
    step = jnp.exp(jnp.sum(jnp.where(eye8, jnp.broadcast_to(v_step[...], (GRP, GRP)), 0.0), axis=1, keepdims=True))
    rate, rot = v_rate[...], v_rot[...]
    real = -rate
    magnitude = jnp.exp(real * step)
    angle = rot * step
    decay_re = magnitude * jnp.cos(angle)
    decay_im = magnitude * jnp.sin(angle)
    denominator = real * real + rot * rot
    lift_re = ((decay_re - 1.0) * real + decay_im * rot) / denominator
    lift_im = (decay_im * real - (decay_re - 1.0) * rot) / denominator
    bd_hi[...] = jnp.zeros_like(bd_hi)
    bd_lo[...] = jnp.zeros_like(bd_lo)
    rbd[...] = jnp.zeros_like(rbd)
    fresh[...] = jnp.zeros_like(fresh)
    for g in range(GRP):
        rows = slice(g * GCH, (g + 1) * GCH)
        l_re, l_im = lift_re[g:g + 1, :], lift_im[g:g + 1, :]
        b_re, b_im = v_inre[rows, :], v_inim[rows, :]
        for n, value in enumerate((l_re * b_re - l_im * b_im, l_re * b_im + l_im * b_re)):
            lanes = slice((2 * g + n) * 128, (2 * g + n) * 128 + STATE)
            hi = value.astype(BF)
            bd_hi[rows, lanes] = hi
            bd_lo[rows, lanes] = (value - hi.astype(F32)).astype(BF)
        rbd[rows, (2 * g) * 128:(2 * g) * 128 + STATE] = v_rre[rows, :].astype(BF)
        rbd[rows, (2 * g + 1) * 128:(2 * g + 1) * 128 + STATE] = (-v_rim[rows, :]).astype(BF)
    tiler = (iota((GCH, 128), 0) == lax.rem(iota((GCH, 128), 1), GCH)).astype(BF)
    skip_hi = v_skip[...].astype(BF)
    skip_rest = v_skip[...] - skip_hi.astype(F32)
    skip_mid = skip_rest.astype(BF)
    skip_lo = (skip_rest - skip_mid.astype(F32)).astype(BF)
    skip_rep = dot(skip_hi, tiler) + dot(skip_mid, tiler) + dot(skip_lo, tiler)
    skip_row = jnp.sum(
        jnp.where(lax.div(iota((GRP, 128), 1), GCH) == iota((GRP, 128), 0), skip_rep, 0.0), axis=0, keepdims=True
    )
    r0, r1 = v_routes[0:1, :], v_routes[1:2, :]
    oh0 = (r0 == iota((NEP, ROWS), 0)).astype(F32)
    oh1 = (r1 == iota((NEP, ROWS), 0)).astype(F32)
    upper_tri = (iota((ROWS, ROWS), 0) < iota((ROWS, ROWS), 1)).astype(BF)
    before = dot((oh0 + oh1).astype(BF), upper_tri)
    dest0 = r0.astype(F32) * SLOT + jnp.sum(before * oh0, axis=0, keepdims=True)
    dest1 = r1.astype(F32) * SLOT + jnp.sum(before * oh1, axis=0, keepdims=True)
    place = iota((SLOTS, ROWS), 0).astype(F32)
    m0, m1 = (dest0 == place).astype(F32), (dest1 == place).astype(F32)
    d_map[...] = (m0 + m1).astype(BF)
    w_all = jnp.transpose(v_weights[0:1, :] * m0 + v_weights[1:2, :] * m1)
    w_hi = w_all.astype(BF)
    wt[0] = w_hi
    wt[1] = (w_all - w_hi.astype(F32)).astype(BF)

    loads[1].wait()
    loads[2].wait()

    total = [None, None]

    def mix_block(t):
        rows = g1[t].astype(F32)
        squares = jnp.sum(rows * rows, axis=1, keepdims=True)
        gain = v_mix[:, pl.ds(pl.multiple_of(t * WIDTH, WIDTH), WIDTH)]
        product = dot((rows * gain).astype(BF), v_win[pl.ds(pl.multiple_of(t * WIDTH, WIDTH), WIDTH), :])
        total[0] = squares if total[0] is None else total[0] + squares
        total[1] = product if total[1] is None else total[1] + product

    mix_block(tp)
    gather_relay(*one)
    mix_block(down)
    mix_block(up)
    arrive(at1(partner, 0, ROWS), g1_s.at[4], g1_r.at[4])
    mix_block(partner)
    gather_far(*one)
    arrive(at1(down_oc, 0, ROWS), g1_s.at[5], g1_r.at[5])
    mix_block(down_oc)
    arrive(at1(up_oc, 0, ROWS), g1_s.at[6], g1_r.at[6])
    mix_block(up_oc)
    mix_block(far)
    arrive(at1(far_oc, 0, ROWS // 2), g1_s.at[7], g1_r.at[7])
    arrive(at1(far_oc, ROWS // 2, ROWS // 2), g1_s.at[8], g1_r.at[8])
    mix_block(far_oc)
    u_in = (total[1] * lax.rsqrt(total[0] / (NTP * WIDTH) + EPS)).astype(BF)

    drive = dot(u_in, bd_hi[...]) + dot(u_in, bd_lo[...])
    for g in range(GRP):
        old_re = v_state[pl.ds(g, ROWS, stride=2 * GRP), :]
        old_im = v_state[pl.ds(GRP + g, ROWS, stride=2 * GRP), :]
        k_re, k_im = decay_re[g:g + 1, :], decay_im[g:g + 1, :]
        new_re = k_re * old_re - k_im * old_im + drive[:, (2 * g) * 128:(2 * g) * 128 + STATE]
        new_im = k_re * old_im + k_im * old_re + drive[:, (2 * g + 1) * 128:(2 * g + 1) * 128 + STATE]
        state_out[pl.ds(g, ROWS, stride=2 * GRP), :] = new_re
        state_out[pl.ds(GRP + g, ROWS, stride=2 * GRP), :] = new_im
        fresh[:, (2 * g) * 128:(2 * g) * 128 + STATE] = new_re.astype(BF)
        fresh[:, (2 * g + 1) * 128:(2 * g + 1) * 128 + STATE] = new_im.astype(BF)
    act = jax.nn.gelu(dot_nt(fresh[...], rbd[...]) + skip_row * u_in.astype(F32))
    act32[...] = act
    act_all[tp] = act.astype(BF)
    for d in range(1, NTP):
        send(act_all.at[tp], act_all.at[tp], a_s.at[d], a_r.at[d], (ep, lax.rem(tp + d, NTP)))
    loads[14].wait()
    loads[15].wait()
    for d in range(1, NTP):
        arrive(act_all.at[lax.rem(tp + NTP - d, NTP)], a_s.at[d], a_r.at[d])
    logit = dot(jnp.concatenate([act_all[t] for t in range(NTP)], axis=1), v_glu[...])
    mixed[...] = (act32[...] * jax.nn.sigmoid(logit)).astype(BF)

    order = (yo, yp, ym, y)

    def reduce_scatter(product, rows, sets, ds, dr, q, own, rel, dire, mrg, ms, ss, rs, done):
        half = rows // 2
        piece = half // sets
        base = 4

        def lo(i):
            return pl.ds(i * piece, piece)

        def hi(i):
            return pl.ds(half + i * piece, piece)

        def sem(kind, i):
            return base + kind * sets + i

        def to_partner(j):
            ds[j] = product(order[j] * 2 + oc).astype(BF)
            send(ds.at[j], dr.at[j], ss.at[j], rs.at[j], (ep, partner))

        to_partner(0)
        to_partner(1)
        to_partner(2)

        def on_chip(j):
            value = product(order[j] * 2 + c)
            arrive(dr.at[j], ss.at[j], rs.at[j])
            return value + dr[j].astype(F32)

        q[0] = on_chip(0).astype(BF)
        for i in range(sets):
            send(q.at[0, lo(i), :], rel.at[0, lo(i), :], ss.at[sem(0, i)], rs.at[sem(0, i)], (ep, up))
            send(q.at[0, hi(i), :], rel.at[1, lo(i), :], ss.at[sem(1, i)], rs.at[sem(1, i)], (ep, down))
        to_partner(3)
        q[1] = on_chip(1).astype(BF)

        def direct_up(i):
            send(q.at[1, hi(i), :], dire.at[0, lo(i), :], ss.at[sem(2, i)], rs.at[sem(2, i)], (ep, up))

        def direct_down(i):
            send(q.at[2, lo(i), :], dire.at[1, lo(i), :], ss.at[sem(3, i)], rs.at[sem(3, i)], (ep, down))

        direct_up(0)
        q[2] = on_chip(2).astype(BF)
        direct_down(0)
        own[...] = on_chip(3)
        for i in range(sets):
            if i:
                direct_up(i)
                direct_down(i)
            arrive(rel.at[0, lo(i), :], ss.at[sem(0, i)], rs.at[sem(0, i)])
            ms[0, i * piece:(i + 1) * piece, :] = (
                q[1, i * piece:(i + 1) * piece, :].astype(F32) + rel[0, i * piece:(i + 1) * piece, :].astype(F32)
            ).astype(BF)
            send(ms.at[0, lo(i), :], mrg.at[0, lo(i), :], ss.at[sem(4, i)], rs.at[sem(4, i)], (ep, up))
            arrive(rel.at[1, lo(i), :], ss.at[sem(1, i)], rs.at[sem(1, i)])
            ms[1, i * piece:(i + 1) * piece, :] = (
                q[2, half + i * piece:half + (i + 1) * piece, :].astype(F32)
                + rel[1, i * piece:(i + 1) * piece, :].astype(F32)
            ).astype(BF)
            send(ms.at[1, lo(i), :], mrg.at[1, lo(i), :], ss.at[sem(5, i)], rs.at[sem(5, i)], (ep, down))
        for i in range(sets):
            part = slice(i * piece, (i + 1) * piece)
            arrive(dire.at[1, lo(i), :], ss.at[sem(3, i)], rs.at[sem(3, i)])
            arrive(mrg.at[0, lo(i), :], ss.at[sem(4, i)], rs.at[sem(4, i)])
            done(i * piece, piece, own[part, :] + dire[1, part, :].astype(F32) + mrg[0, part, :].astype(F32))
            top = slice(half + i * piece, half + (i + 1) * piece)
            arrive(dire.at[0, lo(i), :], ss.at[sem(2, i)], rs.at[sem(2, i)])
            arrive(mrg.at[1, lo(i), :], ss.at[sem(5, i)], rs.at[sem(5, i)])
            done(half + i * piece, piece, own[top, :] + dire[0, part, :].astype(F32) + mrg[1, part, :].astype(F32))

    def columns(t):
        return pl.ds(pl.multiple_of(t * WIDTH, WIDTH), WIDTH)

    def branch_done(first, size, value):
        source = g1[tp, first:first + size, :].astype(F32)
        after[first:first + size, :] = (source + value).astype(BF)

    reduce_scatter(
        lambda t: dot(mixed[...], v_out[:, columns(t)]), ROWS, 1,
        b_ds, b_dr, b_q, b_own, b_rel, b_dir, b_mrg, b_ms, b_s, b_r, branch_done,
    )

    outb[...] = dot(d_map[...], after[...]).astype(BF)

    def slot(e):
        return pl.ds(pl.multiple_of(e * SLOT, SLOT), SLOT)

    hops = [(dz, dx) for dz in (0, 1, 3, 2) for dx in (1, 3, 2, 0) if (dz, dx) != (0, 0)]
    for dz, dx in hops:
        k = dz * 4 + dx
        e = lax.rem(z + dz, 4) * 4 + lax.rem(x + dx, 4)
        send(outb.at[slot(e), :], g2.at[tp, slot(ep), :], x_s.at[k], x_r.at[k], (e, tp))
    g2[tp, slot(ep), :] = outb[slot(ep), :]
    loads[16].wait()
    loads[17].wait()
    loads[18].wait()

    def at2(t, first, size):
        return g2.at[t, pl.ds(first, size), :]

    def sems2(table, j):
        return lambda k: table.at[j, k]

    chunk = SLOTS // 4
    turns = (0, 1, 3, 2)
    plans = []
    for j, dz in enumerate(turns):
        first = pl.multiple_of(lax.rem(z + 4 - dz, 4) * chunk, chunk)
        plans.append((at2, chunk // 2, sems2(g2_s, j), sems2(g2_r, j), (first, chunk)))

    def start_chunk(j):
        dz = turns[j]
        for dx in (1, 3, 2, 0):
            if (dz, dx) == (0, 0):
                continue
            k = dz * 4 + dx
            s = lax.rem(z + 4 - dz, 4) * 4 + lax.rem(x + 4 - dx, 4)
            arrive(g2.at[tp, slot(s), :], x_s.at[k], x_r.at[k])
        gather_send(*plans[j])

    began = []

    def expert_block(t):
        gain = v_ffn[:, columns(t)]
        rows = g2[t].astype(F32)
        scaled = (rows * gain).astype(BF)
        squares = rows * rows
        squares = squares[:, 0:128] + squares[:, 128:256] + squares[:, 256:384] + squares[:, 384:512]
        gate, upper = dot_nt(scaled, v_gate[:, columns(t)]), dot_nt(scaled, v_up[:, columns(t)])
        if began:
            sq[...] += squares
            acc_g[...] += gate
            acc_u[...] += upper
        else:
            began.append(True)
            sq[...] = squares
            acc_g[...] = gate
            acc_u[...] = upper

    def from_partner(t, kinds):
        for j in range(4):
            at, half, ss, rs, (first, size) = plans[j]
            if len(kinds) == 1:
                arrive(at(t, first, size), ss(kinds[0]), rs(kinds[0]))
            else:
                arrive(at(t, first, half), ss(kinds[0]), rs(kinds[0]))
                arrive(at(t, first + half, half), ss(kinds[1]), rs(kinds[1]))

    for j in range(4):
        start_chunk(j)
    expert_block(tp)
    gather_relay(*plans[0])
    from_partner(partner, (4,))
    expert_block(partner)
    for j in range(1, 4):
        gather_relay(*plans[j])
    expert_block(down)
    gather_far(*plans[0])
    expert_block(up)
    gather_far(*plans[1])
    from_partner(down_oc, (5,))
    expert_block(down_oc)
    gather_far(*plans[2])
    from_partner(up_oc, (6,))
    expert_block(up_oc)
    gather_far(*plans[3])
    expert_block(far)
    from_partner(far_oc, (7, 8))
    expert_block(far_oc)

    loads[19].wait()
    for r in range(0, SLOTS, 64):
        scale = lax.rsqrt(jnp.sum(sq[r:r + 64, :], axis=1, keepdims=True) / (NTP * WIDTH) + EPS)
        gate, upper = acc_g[r:r + 64, :] * scale, acc_u[r:r + 64, :] * scale
        hidden[r:r + 64, :] = (gate * jax.nn.sigmoid(gate) * upper).astype(BF)

    def expert_done(first, size, value):
        eout[first:first + size, :] = value.astype(BF)
        for s in range(first // SLOT, (first + size) // SLOT):
            rows = slice(s * SLOT, (s + 1) * SLOT)

            @pl.when(ep == s)
            def _():
                back[rows, :] = eout[rows, :]

            @pl.when(ep != s)
            def _():
                pltpu.make_async_remote_copy(
                    src_ref=eout.at[pl.ds(s * SLOT, SLOT), :], dst_ref=back.at[slot(ep), :],
                    send_sem=ret_s.at[s], recv_sem=ret_r.at[ep], device_id=(s, tp), device_id_type=MESH,
                ).start()

    reduce_scatter(
        lambda t: dot(hidden[...], v_down[:, columns(t)]), SLOTS, 2,
        e_ds, e_dr, e_q, e_own, e_rel, e_dir, e_mrg, e_ms, e_s, e_r, expert_done,
    )
    for d in range(1, NEP):
        e = lax.rem(ep + d, NEP)
        arrive(back.at[slot(e), :], ret_s.at[e], ret_r.at[e])
    combined = dot(wt[0], back[...]) + dot(wt[1], back[...])
    out[...] = (after[...].astype(F32) + combined).astype(BF)
    for copy in sent:
        copy.wait_send()
    for d in range(1, NEP):
        e = lax.rem(ep + d, NEP)
        pltpu.make_async_remote_copy(
            src_ref=eout.at[slot(e), :], dst_ref=eout.at[slot(e), :], send_sem=ret_s.at[e], recv_sem=ret_r.at[e],
            device_id=(e, tp), device_id_type=MESH,
        ).wait_send()


def write_out(layer, state, layer_hbm, state_hbm, sems):
    copies = [pltpu.make_async_copy(state, state_hbm, sems.at[0]), pltpu.make_async_copy(layer, layer_hbm, sems.at[1])]
    for copy in copies:
        copy.start()
    for copy in copies:
        copy.wait()


def per_device(
    residual, routes, route_weights, state_prev, mix_gain, ffn_gain, w_in, decay_rate, rotation,
    log_step, in_re, in_im, read_re, read_im, skip_gain, w_glu, w_out, w_gate, w_up, w_down,
):
    dma = pltpu.SemaphoreType.DMA
    vm = pltpu.VMEM
    operands = (
        residual, routes.T, route_weights.T, state_prev.reshape(ROWS * 2 * GRP, STATE), mix_gain.reshape(1, -1),
        ffn_gain.reshape(1, -1), w_in, decay_rate, rotation, log_step.reshape(1, GRP),
        in_re.transpose(0, 2, 1).reshape(GRP * GCH, STATE), in_im.transpose(0, 2, 1).reshape(GRP * GCH, STATE), read_re.reshape(GRP * GCH, STATE),
        read_im.reshape(GRP * GCH, STATE), skip_gain, w_glu, w_out, w_gate[0].T, w_up[0].T, w_down[0],
    )

    def exchange(rows):
        half = rows // 2
        return [
            vm((4, rows, WIDTH), BF), vm((4, rows, WIDTH), BF), vm((3, rows, WIDTH), BF), vm((rows, WIDTH), F32),
            vm((2, half, WIDTH), BF), vm((2, half, WIDTH), BF), vm((2, half, WIDTH), BF), vm((2, half, WIDTH), BF),
        ]

    scratch = [vm(operands[i].shape, operands[i].dtype) for i in range(1, 20)]
    scratch += [
        vm((NTP, ROWS, WIDTH), BF), vm((128, 2048), BF), vm((128, 2048), BF),
        vm((128, 2048), BF), vm((ROWS, 2048), BF), vm((NTP, ROWS, 128), BF),
        vm((ROWS, 128), F32), vm((ROWS, 128), BF),
    ]
    scratch += exchange(ROWS)
    scratch += [
        vm((ROWS, WIDTH), BF), vm((SLOTS, ROWS), BF), vm((2, ROWS, SLOTS), BF), vm((SLOTS, WIDTH), BF),
        vm((NTP, SLOTS, WIDTH), BF), vm((SLOTS, FFW), F32), vm((SLOTS, FFW), F32), vm((SLOTS, 128), F32),
        vm((SLOTS, FFW), BF),
    ]
    scratch += exchange(SLOTS)
    scratch += [vm((SLOTS, WIDTH), BF), vm((SLOTS, WIDTH), BF)]
    scratch += [
        dma((20,)), dma((9,)), dma((9,)), dma((8,)), dma((8,)), dma((10,)), dma((10,)), dma((16,)), dma((16,)),
        dma((4, 9)), dma((4, 9)), dma((16,)), dma((16,)), dma((16,)), dma((16,)),
    ]
    anywhere = pl.BlockSpec(memory_space=pltpu.HBM)
    outside = pl.BlockSpec(memory_space=pl.ANY)
    inside = pl.BlockSpec(memory_space=pltpu.VMEM)
    layer_out, state_next = pl.pallas_call(
        kernel,
        out_shape=(vm((ROWS, WIDTH), BF), vm((ROWS * 2 * GRP, STATE), F32)),
        in_specs=[anywhere] * 20,
        out_specs=(inside, inside),
        scratch_shapes=scratch,
        compiler_params=pltpu.CompilerParams(
            collective_id=0, has_side_effects=True, vmem_limit_bytes=44 * 1024 * 1024
        ),
        name="layer",
    )(*[pltpu.with_memory_space_constraint(a, pltpu.HBM) for a in operands])
    layer_out = pltpu.with_memory_space_constraint(layer_out, pltpu.VMEM)
    state_next = pltpu.with_memory_space_constraint(state_next, pltpu.VMEM)
    layer_out, state_next = pl.pallas_call(
        write_out,
        out_shape=(
            jax.ShapeDtypeStruct((ROWS, WIDTH), BF),
            jax.ShapeDtypeStruct((ROWS * 2 * GRP, STATE), F32),
        ),
        in_specs=[inside] * 2,
        out_specs=(outside, outside),
        scratch_shapes=[dma((2,))],
        name="write_out",
    )(layer_out, state_next)
    return layer_out, state_next.reshape(ROWS, 2, GRP, STATE)


def solution(mesh):
    return jax.shard_map(
        per_device,
        mesh=mesh,
        in_specs=(
            P("ep", "tp"), P("ep", None), P("ep", None), P("ep", None, "tp", None), P(), P(), P(None, "tp"),
            P("tp", None), P("tp", None), P("tp"), P("tp", None, None), P("tp", None, None), P("tp", None, None),
            P("tp", None, None), P("tp", None), P(None, "tp"), P("tp", None), P("ep", None, "tp"),
            P("ep", None, "tp"), P("ep", "tp", None),
        ),
        out_specs=(P("ep", "tp"), P("ep", None, "tp", None)),
        check_vma=False,
    )
```

```python
import functools

import jax
import jax.numpy as jnp
from jax import lax
from jax.experimental import pallas as pl
from jax.experimental.pallas import tpu as pltpu
from jax.sharding import PartitionSpec as P

MESH = pl.DeviceIdType.MESH
BF = jnp.bfloat16
F32 = jnp.float32
EPS = 1e-06
NT = (((1,), (1,)), ((), ()))

NEP = 16
NTP = 8
ROWS = 64
WIDTH = 512
SLOT = 16
SLOTS = NEP * SLOT
FFW = 704
STATE = 64
GRP = 8
GCH = 16


def dot(a, b):
    return jnp.dot(a, b, preferred_element_type=F32)


def dot_nt(a, b):
    return lax.dot_general(a, b, NT, preferred_element_type=F32)


def iota(shape, dim):
    return lax.broadcasted_iota(jnp.int32, shape, dim)


def kernel(
    residual, routes, weights, state, mix_gain, ffn_gain, w_in, decay_rate, rotation,
    log_step, in_re, in_im, read_re, read_im, skip, w_glu, w_out, w_gate, w_up, w_down,
    out, state_out,
    v_routes, v_weights, v_state, v_gain, v_win, v_lam, v_step, v_io, v_skip, v_glu, v_out, v_gu, v_down,
    g1, bd_hi, bd_lo, rbd, fresh, act_all, act32, mixed,
    b_q, b_own, b_rel, b_dir, b_mrg, b_ms,
    v_glu2, wo2, after, d_map, wt, outb, g2, acc_g, acc_u, sq, hidden,
    e_ds, e_dr, e_q, e_own, e_rel, e_dir, e_mrg, e_ms, eout, back,
    load_sem, send_sem, g1_r, a_r, b_r, d_r, x_r, g2_r, e_r, ret_r,
):
    ep = lax.axis_index("ep")
    tp = lax.axis_index("tp")
    y, c = lax.div(tp, 2), lax.rem(tp, 2)
    z, x = lax.div(ep, 4), lax.rem(ep, 4)
    yp, ym, yo = lax.rem(y + 1, 4), lax.rem(y + 3, 4), lax.rem(y + 2, 4)
    oc = 1 - c
    partner = y * 2 + oc
    up, down = yp * 2 + c, ym * 2 + c
    def send(src, dst, exchange, rs, device):
        pltpu.make_async_remote_copy(
            src_ref=src, dst_ref=dst, send_sem=send_sem.at[exchange], recv_sem=rs, device_id=device, device_id_type=MESH
        ).start()

    def remote(ref, exchange, rs):
        return pltpu.make_async_remote_copy(
            src_ref=ref, dst_ref=ref, send_sem=send_sem.at[exchange], recv_sem=rs, device_id=(ep, partner),
            device_id_type=MESH,
        )

    def arrive(dst, rs):
        remote(dst, 0, rs).wait_recv()

    def left(ref, exchange):
        remote(ref, exchange, g1_r.at[0]).wait_send()

    groups = [
        [(residual, g1.at[tp])],
        [(w_in, v_win)],
        [(mix_gain, v_gain.at[0]), (ffn_gain, v_gain.at[1])],
        [(decay_rate, v_lam.at[0]), (rotation, v_lam.at[1])],
        [(log_step, v_step)],
        [(in_re, v_io.at[0]), (in_im, v_io.at[1]), (read_re, v_io.at[2]), (read_im, v_io.at[3])],
        [(skip, v_skip)],
        [(routes, v_routes)],
        [(weights, v_weights)],
        [(w_glu, v_glu)],
        [(w_out, v_out)],
        [(state, v_state)],
        [(w_gate, v_gu.at[0]), (w_up, v_gu.at[1])],
        [(w_down, v_down)],
    ]
    wholes = [
        g1.at[tp], v_win, v_gain, v_lam, v_step, v_io, v_skip, v_routes, v_weights, v_glu, v_out, v_state, v_gu, v_down
    ]

    def load(i):
        for src, dst in groups[i]:
            pltpu.make_async_copy(src, dst, load_sem.at[i]).start()

    def loaded(i):
        pltpu.make_async_copy(wholes[i], wholes[i], load_sem.at[i]).wait()

    load(0)

    barrier = pltpu.get_barrier_semaphore()
    for d in range(1, NTP):
        pl.semaphore_signal(barrier, inc=1, device_id=(ep, lax.rem(tp + d, NTP)), device_id_type=MESH)
    for d in range(1, NEP):
        pl.semaphore_signal(barrier, inc=1, device_id=(lax.rem(ep + d, NEP), tp), device_id_type=MESH)

    for i in range(1, len(groups)):
        load(i)

    order = (yo, yp, ym, y)

    def columns(t):
        return pl.ds(pl.multiple_of(t * WIDTH, WIDTH), WIDTH)

    def split_send(buf, half, rs, rows):
        first, size = rows
        lo_half, hi_half = (first, half), (first + half, half)
        send(buf(tp, *lo_half), buf(tp, *lo_half), 0, rs(0), (ep, up))
        send(buf(tp, *hi_half), buf(tp, *hi_half), 0, rs(1), (ep, down))
        send(buf(tp, *hi_half), buf(tp, *hi_half), 0, rs(2), (ep, up))
        send(buf(tp, *lo_half), buf(tp, *lo_half), 0, rs(3), (ep, down))
        send(buf(tp, *rows), buf(tp, *rows), 0, rs(4), (ep, partner))

    def split_relay(buf, half, rs, rows):
        first, size = rows
        lo_half, hi_half = (first, half), (first + half, half)
        arrive(buf(down, *lo_half), rs(0))
        send(buf(down, *lo_half), buf(down, *lo_half), 0, rs(5), (ep, up))
        arrive(buf(up, *hi_half), rs(1))
        send(buf(up, *hi_half), buf(up, *hi_half), 0, rs(5), (ep, down))
        arrive(buf(down, *hi_half), rs(2))
        send(buf(down, *rows), buf(down, *rows), 0, rs(6), (ep, partner))
        arrive(buf(up, *lo_half), rs(3))
        send(buf(up, *rows), buf(up, *rows), 0, rs(7), (ep, partner))

    far, far_oc = yo * 2 + c, yo * 2 + oc
    up_oc, down_oc = yp * 2 + oc, ym * 2 + oc

    def at1(t, first, size):
        return g1.at[t, pl.ds(first, size), :]

    one = (at1, ROWS // 2, lambda k: g1_r.at[k], (0, ROWS))
    loaded(0)
    pl.semaphore_wait(barrier, NTP + NEP - 2)
    split_send(*one)
    for i in range(3, 9):
        loaded(i)

    eye8 = iota((GRP, GRP), 0) == iota((GRP, GRP), 1)
    step = jnp.exp(jnp.sum(jnp.where(eye8, jnp.broadcast_to(v_step[...], (GRP, GRP)), 0.0), axis=1, keepdims=True))
    rate, rot = v_lam[0], v_lam[1]
    real = -rate
    magnitude = jnp.exp(real * step)
    angle = rot * step
    decay_re = magnitude * jnp.cos(angle)
    decay_im = magnitude * jnp.sin(angle)
    denominator = real * real + rot * rot
    lift_re = ((decay_re - 1.0) * real + decay_im * rot) / denominator
    lift_im = (decay_im * real - (decay_re - 1.0) * rot) / denominator
    bd_hi[...] = jnp.zeros_like(bd_hi)
    bd_lo[...] = jnp.zeros_like(bd_lo)
    rbd[...] = jnp.zeros_like(rbd)
    fresh[...] = jnp.zeros_like(fresh)
    for g in range(GRP):
        rows = slice(g * GCH, (g + 1) * GCH)
        l_re, l_im = lift_re[g:g + 1, :], lift_im[g:g + 1, :]
        b_re, b_im = v_io[0, rows, :], v_io[1, rows, :]
        for n, value in enumerate((l_re * b_re - l_im * b_im, l_re * b_im + l_im * b_re)):
            lanes = slice((2 * g + n) * 128, (2 * g + n) * 128 + STATE)
            hi = value.astype(BF)
            bd_hi[rows, lanes] = hi
            bd_lo[rows, lanes] = (value - hi.astype(F32)).astype(BF)
        rbd[rows, (2 * g) * 128:(2 * g) * 128 + STATE] = v_io[2, rows, :].astype(BF)
        rbd[rows, (2 * g + 1) * 128:(2 * g + 1) * 128 + STATE] = (-v_io[3, rows, :]).astype(BF)
    tiler = (iota((GCH, 128), 0) == lax.rem(iota((GCH, 128), 1), GCH)).astype(BF)
    skip_hi = v_skip[...].astype(BF)
    skip_rest = v_skip[...] - skip_hi.astype(F32)
    skip_mid = skip_rest.astype(BF)
    skip_lo = (skip_rest - skip_mid.astype(F32)).astype(BF)
    skip_rep = dot(skip_hi, tiler) + dot(skip_mid, tiler) + dot(skip_lo, tiler)
    skip_row = jnp.sum(
        jnp.where(lax.div(iota((GRP, 128), 1), GCH) == iota((GRP, 128), 0), skip_rep, 0.0), axis=0, keepdims=True
    )
    r0, r1 = v_routes[0:1, :], v_routes[1:2, :]
    oh0 = (r0 == iota((NEP, ROWS), 0)).astype(F32)
    oh1 = (r1 == iota((NEP, ROWS), 0)).astype(F32)
    upper_tri = (iota((ROWS, ROWS), 0) < iota((ROWS, ROWS), 1)).astype(BF)
    before = dot((oh0 + oh1).astype(BF), upper_tri)
    dest0 = r0.astype(F32) * SLOT + jnp.sum(before * oh0, axis=0, keepdims=True)
    dest1 = r1.astype(F32) * SLOT + jnp.sum(before * oh1, axis=0, keepdims=True)
    place = iota((SLOTS, ROWS), 0).astype(F32)
    m0, m1 = (dest0 == place).astype(F32), (dest1 == place).astype(F32)
    d_map[...] = (m0 + m1).astype(BF)
    w_all = jnp.transpose(v_weights[0:1, :] * m0 + v_weights[1:2, :] * m1)
    w_hi = w_all.astype(BF)
    wt[0] = w_hi
    wt[1] = (w_all - w_hi.astype(F32)).astype(BF)

    loaded(1)
    loaded(2)
    loaded(9)
    loaded(10)
    send(v_glu, v_glu2, 1, d_r.at[0], (ep, partner))
    for j in range(4):
        send(v_out.at[:, columns(order[j] * 2 + oc)], wo2.at[j], 2, d_r.at[1], (ep, partner))

    total = [None, None]

    def mix_block(t):
        rows = g1[t].astype(F32)
        squares = jnp.sum(rows * rows, axis=1, keepdims=True)
        gain = v_gain[0, :, columns(t)]
        product = dot((rows * gain).astype(BF), v_win[columns(t), :])
        total[0] = squares if total[0] is None else total[0] + squares
        total[1] = product if total[1] is None else total[1] + product

    mix_block(tp)
    split_relay(*one)
    mix_block(down)
    mix_block(up)
    arrive(g1.at[partner], g1_r.at[4])
    mix_block(partner)
    arrive(g1.at[far], g1_r.at[5])
    send(g1.at[far], g1.at[far], 0, g1_r.at[8], (ep, partner))
    arrive(g1.at[down_oc], g1_r.at[6])
    mix_block(down_oc)
    arrive(g1.at[up_oc], g1_r.at[7])
    mix_block(up_oc)
    mix_block(far)
    arrive(g1.at[far_oc], g1_r.at[8])
    mix_block(far_oc)
    u_in = (total[1] * lax.rsqrt(total[0] / (NTP * WIDTH) + EPS)).astype(BF)

    loaded(11)
    drive = dot(u_in, bd_hi[...]) + dot(u_in, bd_lo[...])
    for g in range(GRP):
        old_re = v_state[pl.ds(g, ROWS, stride=2 * GRP), :]
        old_im = v_state[pl.ds(GRP + g, ROWS, stride=2 * GRP), :]
        k_re, k_im = decay_re[g:g + 1, :], decay_im[g:g + 1, :]
        new_re = k_re * old_re - k_im * old_im + drive[:, (2 * g) * 128:(2 * g) * 128 + STATE]
        new_im = k_re * old_im + k_im * old_re + drive[:, (2 * g + 1) * 128:(2 * g + 1) * 128 + STATE]
        state_out[pl.ds(g, ROWS, stride=2 * GRP), :] = new_re
        state_out[pl.ds(GRP + g, ROWS, stride=2 * GRP), :] = new_im
        fresh[:, (2 * g) * 128:(2 * g) * 128 + STATE] = new_re.astype(BF)
        fresh[:, (2 * g + 1) * 128:(2 * g + 1) * 128 + STATE] = new_im.astype(BF)
    act = jax.nn.gelu(dot_nt(fresh[...], rbd[...]) + skip_row * u_in.astype(F32))
    act32[...] = act
    act_all[tp] = act.astype(BF)
    towards = (far, far_oc, up, down, up_oc, down_oc, partner)
    for t in towards:
        send(act_all.at[tp], act_all.at[tp], 3, a_r.at[0], (ep, t))
    arrive(v_glu2, d_r.at[0])
    arrive(wo2, d_r.at[1])
    arrive(act_all.at[0:NTP - 1], a_r.at[0])
    everything = jnp.concatenate([act_all[t] for t in range(NTP)], axis=1)
    mixed[0] = (act32[...] * jax.nn.sigmoid(dot(everything, v_glu[...]))).astype(BF)
    mixed[1] = (act_all[partner].astype(F32) * jax.nn.sigmoid(dot(everything, v_glu2[...]))).astype(BF)

    def scatter(q, rel, dire, mrg, ms, exchange, rs, base, piece, lo, hi):
        low, high = pl.ds(lo, piece), pl.ds(hi, piece)

        def far_blocks():
            send(q.at[0, low, :], rel.at[0], exchange, rs.at[base], (ep, up))
            send(q.at[0, high, :], rel.at[1], exchange, rs.at[base + 1], (ep, down))

        def near_up():
            send(q.at[1, high, :], dire.at[0], exchange, rs.at[base + 2], (ep, up))

        def near_down():
            send(q.at[2, low, :], dire.at[1], exchange, rs.at[base + 3], (ep, down))

        def merge():
            arrive(rel.at[0], rs.at[base])
            ms[0] = (q[1, lo:lo + piece, :].astype(F32) + rel[0].astype(F32)).astype(BF)
            send(ms.at[0], mrg.at[0], exchange, rs.at[base + 4], (ep, up))
            arrive(rel.at[1], rs.at[base + 1])
            ms[1] = (q[2, hi:hi + piece, :].astype(F32) + rel[1].astype(F32)).astype(BF)
            send(ms.at[1], mrg.at[1], exchange, rs.at[base + 5], (ep, down))

        def final(own, done):
            arrive(dire.at[1], rs.at[base + 3])
            arrive(mrg.at[0], rs.at[base + 4])
            done(0, own[lo:lo + piece, :] + dire[1].astype(F32) + mrg[0].astype(F32))
            arrive(dire.at[0], rs.at[base + 2])
            arrive(mrg.at[1], rs.at[base + 5])
            done(1, own[hi:hi + piece, :] + dire[0].astype(F32) + mrg[1].astype(F32))

        return far_blocks, near_up, near_down, merge, final

    def branch_done(part, value):
        rows = slice(part * (ROWS // 2), (part + 1) * (ROWS // 2))
        after[rows, :] = (g1[tp, rows, :].astype(F32) + value).astype(BF)

    def chip_product(j):
        return dot(mixed[0], v_out[:, columns(order[j] * 2 + c)]) + dot(mixed[1], wo2[j])

    far_blocks, near_up, near_down, merge, final = scatter(
        b_q, b_rel, b_dir, b_mrg, b_ms, 4, b_r, 0, ROWS // 2, 0, ROWS // 2
    )
    b_q[0] = chip_product(0).astype(BF)
    far_blocks()
    b_q[1] = chip_product(1).astype(BF)
    near_up()
    b_q[2] = chip_product(2).astype(BF)
    near_down()
    b_own[...] = chip_product(3)
    merge()
    final(b_own, branch_done)

    outb[...] = dot(d_map[...], after[...]).astype(BF)

    def slot(e):
        return pl.ds(pl.multiple_of(e * SLOT, SLOT), SLOT)

    turns = (2, 3, 1, 0)
    chunk = SLOTS // 4
    across = (2, 1, 3, 0)

    def spot(j, xx):
        return pl.ds(pl.multiple_of(j * chunk + xx * SLOT, SLOT), SLOT)

    def rows_of(j):
        return pl.ds(j * chunk, chunk)

    for j in (3, 2, 1, 0):
        dz = turns[j]
        for dx in across:
            if (dz, dx) != (0, 0):
                e = lax.rem(z + dz, 4) * 4 + lax.rem(x + dx, 4)
                send(outb.at[slot(e), :], g2.at[tp, spot(j, x), :], 5, x_r.at[j], (e, tp))
    g2[tp, spot(3, x), :] = outb[slot(ep), :]
    loaded(12)

    def start_chunk(j):
        arrive(g2.at[tp, pl.ds(j * chunk, chunk if turns[j] else chunk - SLOT), :], x_r.at[j])
        block = g2.at[tp, rows_of(j), :]
        send(block, block, 6, g2_r.at[j], (ep, up))
        send(block, block, 6, g2_r.at[4 + j], (ep, down))
        send(block, block, 6, g2_r.at[12], (ep, partner))

    def relay(j):
        first = g2.at[down, rows_of(j), :]
        arrive(first, g2_r.at[j])
        low = g2.at[down, pl.ds(j * chunk, chunk // 2), :]
        send(low, low, 6, g2_r.at[8 + j], (ep, up))
        send(first, first, 6, g2_r.at[13], (ep, partner))
        second = g2.at[up, rows_of(j), :]
        arrive(second, g2_r.at[4 + j])
        high = g2.at[up, pl.ds(j * chunk + chunk // 2, chunk // 2), :]
        send(high, high, 6, g2_r.at[8 + j], (ep, down))
        send(second, second, 6, g2_r.at[14], (ep, partner))

    def pass_far(j):
        block = g2.at[far, rows_of(j), :]
        arrive(block, g2_r.at[8 + j])
        send(block, block, 6, g2_r.at[15], (ep, partner))

    def expert_block(t, first=False):
        rows = g2[t].astype(F32)
        scaled = (rows * v_gain[1, :, columns(t)]).astype(BF)
        squares = rows * rows
        squares = squares[:, 0:128] + squares[:, 128:256] + squares[:, 256:384] + squares[:, 384:512]
        gate, upper = dot_nt(scaled, v_gu[0, :, columns(t)]), dot_nt(scaled, v_gu[1, :, columns(t)])
        if first:
            sq[...] = squares
            acc_g[...] = gate
            acc_u[...] = upper
        else:
            sq[...] += squares
            acc_g[...] += gate
            acc_u[...] += upper

    def from_partner(t, k):
        arrive(g2.at[t], g2_r.at[k])
        expert_block(t)

    for j in (3, 2, 1, 0):
        start_chunk(j)
    expert_block(tp, True)
    relay(3)
    from_partner(partner, 12)
    relay(2)
    relay(1)
    relay(0)
    expert_block(down)
    pass_far(3)
    expert_block(up)
    pass_far(2)
    from_partner(down_oc, 13)
    pass_far(1)
    from_partner(up_oc, 14)
    pass_far(0)
    expert_block(far)
    from_partner(far_oc, 15)

    for r in range(0, SLOTS, 64):
        scale = lax.rsqrt(jnp.sum(sq[r:r + 64, :], axis=1, keepdims=True) / (NTP * WIDTH) + EPS)
        gate, upper = acc_g[r:r + 64, :] * scale, acc_u[r:r + 64, :] * scale
        hidden[r:r + 64, :] = (gate * jax.nn.sigmoid(gate) * upper).astype(BF)
    loaded(13)

    def product(t):
        return dot(hidden[...], v_down[:, columns(t)])

    def to_partner(j):
        e_ds[j] = product(order[j] * 2 + oc).astype(BF)
        send(e_ds.at[j], e_dr.at[j], 7, e_r.at[j], (ep, partner))

    def on_chip(j):
        value = product(order[j] * 2 + c)
        arrive(e_dr.at[j], e_r.at[j])
        return value + e_dr[j].astype(F32)

    def expert_done(i):
        def done(part, value):
            j = 2 * part + i
            eout[j * chunk:(j + 1) * chunk, :] = value.astype(BF)
            dz = turns[j]
            for dx in across:
                from_x = lax.rem(x + 4 - dx, 4)
                here = spot(j, from_x)
                if dz or dx:
                    s = lax.rem(z + 4 - dz, 4) * 4 + from_x
                    send(eout.at[here, :], back.at[slot(ep), :], 9, ret_r.at[0], (s, tp))
                else:
                    back[slot(ep), :] = eout[here, :]
        return done

    stages = [
        scatter(
            e_q, e_rel.at[i], e_dir.at[i], e_mrg.at[i], e_ms.at[i], 8, e_r, 4 + 6 * i, chunk, i * chunk, (2 + i) * chunk
        )
        for i in range(2)
    ]
    to_partner(0)
    to_partner(1)
    to_partner(2)
    e_q[0] = on_chip(0).astype(BF)
    stages[0][0]()
    stages[1][0]()
    to_partner(3)
    e_q[1] = on_chip(1).astype(BF)
    stages[0][1]()
    e_q[2] = on_chip(2).astype(BF)
    stages[0][2]()
    e_own[...] = on_chip(3)
    stages[0][3]()
    stages[1][1]()
    stages[1][2]()
    stages[1][3]()
    stages[0][4](e_own, expert_done(0))
    stages[1][4](e_own, expert_done(1))
    arrive(back.at[0:SLOTS - SLOT, :], ret_r.at[0])
    combined = dot(wt[0], back[...]) + dot(wt[1], back[...])
    out[...] = (after[...].astype(F32) + combined).astype(BF)
    left(g1.at[0:NTP - 1], 0)
    left(v_glu, 1)
    left(wo2, 2)
    left(act_all.at[0:NTP - 1], 3)
    left(b_q, 4)
    left(outb.at[0:SLOTS - SLOT, :], 5)
    left(g2.at[0:NTP - 1], 6)
    left(e_ds, 7)
    left(e_q, 8)
    left(eout.at[0:SLOTS - SLOT, :], 9)


def write_out(layer, state, layer_hbm, state_hbm, sems):
    copies = [pltpu.make_async_copy(state, state_hbm, sems.at[0]), pltpu.make_async_copy(layer, layer_hbm, sems.at[1])]
    for copy in copies:
        copy.start()
    for copy in copies:
        copy.wait()


def per_device(
    residual, routes, route_weights, state_prev, mix_gain, ffn_gain, w_in, decay_rate, rotation,
    log_step, in_re, in_im, read_re, read_im, skip_gain, w_glu, w_out, w_gate, w_up, w_down,
):
    dma = pltpu.SemaphoreType.DMA
    vm = pltpu.VMEM
    operands = (
        residual, routes.T, route_weights.T, state_prev.reshape(ROWS * 2 * GRP, STATE), mix_gain.reshape(1, -1),
        ffn_gain.reshape(1, -1), w_in, decay_rate, rotation, log_step.reshape(1, GRP),
        in_re.transpose(0, 2, 1).reshape(GRP * GCH, STATE), in_im.transpose(0, 2, 1).reshape(GRP * GCH, STATE), read_re.reshape(GRP * GCH, STATE),
        read_im.reshape(GRP * GCH, STATE), skip_gain, w_glu, w_out, w_gate[0].T, w_up[0].T, w_down[0],
    )

    def exchange(lead, rows, part):
        return [vm((3, rows, WIDTH), BF), vm((rows, WIDTH), F32)] + [vm((*lead, 2, part, WIDTH), BF)] * 4

    scratch = [
        vm((2, ROWS), jnp.int32), vm((2, ROWS), F32), vm((ROWS * 2 * GRP, STATE), F32), vm((2, 1, NTP * WIDTH), F32),
        vm((NTP * WIDTH, 128), BF), vm((2, GRP, STATE), F32), vm((1, GRP), F32), vm((4, GRP * GCH, STATE), F32),
        vm((GRP, GCH), F32), vm((NEP * ROWS, 128), BF), vm((128, NTP * WIDTH), BF), vm((2, FFW, NTP * WIDTH), BF),
        vm((FFW, NTP * WIDTH), BF),
    ]
    scratch += [
        vm((NTP, ROWS, WIDTH), BF), vm((128, 2048), BF), vm((128, 2048), BF),
        vm((128, 2048), BF), vm((ROWS, 2048), BF), vm((NTP, ROWS, 128), BF),
        vm((ROWS, 128), F32), vm((2, ROWS, 128), BF),
    ]
    scratch += exchange((), ROWS, ROWS // 2)
    scratch += [
        vm((NEP * ROWS, 128), BF), vm((4, 128, WIDTH), BF),
        vm((ROWS, WIDTH), BF), vm((SLOTS, ROWS), BF), vm((2, ROWS, SLOTS), BF), vm((SLOTS, WIDTH), BF),
        vm((NTP, SLOTS, WIDTH), BF), vm((SLOTS, FFW), F32), vm((SLOTS, FFW), F32), vm((SLOTS, 128), F32),
        vm((SLOTS, FFW), BF),
    ]
    scratch += [vm((4, SLOTS, WIDTH), BF)] * 2 + exchange((2,), SLOTS, SLOTS // 4)
    scratch += [vm((SLOTS, WIDTH), BF), vm((SLOTS, WIDTH), BF)]
    scratch += [
        dma((14,)), dma((10,)), dma((9,)), dma((1,)), dma((6,)), dma((2,)), dma((4,)), dma((16,)), dma((16,)), dma((1,))
    ]
    anywhere = pl.BlockSpec(memory_space=pltpu.HBM)
    outside = pl.BlockSpec(memory_space=pl.ANY)
    inside = pl.BlockSpec(memory_space=pltpu.VMEM)
    layer_out, state_next = pl.pallas_call(
        kernel,
        out_shape=(vm((ROWS, WIDTH), BF), vm((ROWS * 2 * GRP, STATE), F32)),
        in_specs=[anywhere] * 20,
        out_specs=(inside, inside),
        scratch_shapes=scratch,
        compiler_params=pltpu.CompilerParams(
            collective_id=0, has_side_effects=True, vmem_limit_bytes=44 * 1024 * 1024
        ),
        name="layer",
    )(*[pltpu.with_memory_space_constraint(a, pltpu.HBM) for a in operands])
    layer_out = pltpu.with_memory_space_constraint(layer_out, pltpu.VMEM)
    state_next = pltpu.with_memory_space_constraint(state_next, pltpu.VMEM)
    layer_out, state_next = pl.pallas_call(
        write_out,
        out_shape=(
            jax.ShapeDtypeStruct((ROWS, WIDTH), BF),
            jax.ShapeDtypeStruct((ROWS * 2 * GRP, STATE), F32),
        ),
        in_specs=[inside] * 2,
        out_specs=(outside, outside),
        scratch_shapes=[dma((2,))],
        name="write_out",
    )(layer_out, state_next)
    return layer_out, state_next.reshape(ROWS, 2, GRP, STATE)


def solution(mesh):
    return jax.shard_map(
        per_device,
        mesh=mesh,
        in_specs=(
            P("ep", "tp"), P("ep", None), P("ep", None), P("ep", None, "tp", None), P(), P(), P(None, "tp"),
            P("tp", None), P("tp", None), P("tp"), P("tp", None, None), P("tp", None, None), P("tp", None, None),
            P("tp", None, None), P("tp", None), P(None, "tp"), P("tp", None), P("ep", None, "tp"),
            P("ep", None, "tp"), P("ep", "tp", None),
        ),
        out_specs=(P("ep", "tp"), P("ep", None, "tp", None)),
        check_vma=False,
    )
```

```python
import functools

import jax
import jax.numpy as jnp
from jax import lax
from jax.experimental import pallas as pl
from jax.experimental.pallas import tpu as pltpu
from jax.sharding import PartitionSpec as P

MESH = pl.DeviceIdType.MESH
BF = jnp.bfloat16
F32 = jnp.float32
EPS = 1e-06
NT = (((1,), (1,)), ((), ()))

NEP = 16
NTP = 8
ROWS = 64
WIDTH = 512
SLOT = 16
SLOTS = NEP * SLOT
FFW = 704
STATE = 64
GRP = 8
GCH = 16


def dot(a, b):
    return jnp.dot(a, b, preferred_element_type=F32)


def dot_nt(a, b):
    return lax.dot_general(a, b, NT, preferred_element_type=F32)


def iota(shape, dim):
    return lax.broadcasted_iota(jnp.int32, shape, dim)


def kernel(
    residual, routes, weights, state, mix_gain, ffn_gain, w_in, decay_rate, rotation,
    log_step, in_re, in_im, read_re, read_im, skip, w_glu, w_out, w_gate, w_up, w_down,
    out, state_out,
    v_routes, v_weights, v_state, v_gain, v_win, v_lam, v_step, v_io, v_skip, v_glu, v_out, v_gu, v_down,
    g1, thru, bd_hi, bd_lo, rbd, fresh, act_all, act32, mixed,
    b_q, b_own, b_rel, b_dir, b_mrg, b_ms,
    v_glu2, wo2, after, d_map, wt, outb, g2, acc_g, acc_u, sq, hidden,
    e_ds, e_dr, e_q, e_own, e_rel, e_dir, e_mrg, e_ms, eout, back,
    load_sem, send_sem, g1_r, a_r, b_r, d_r, x_r, g2_r, e_r, ret_r,
):
    ep = lax.axis_index("ep")
    tp = lax.axis_index("tp")
    y, c = lax.div(tp, 2), lax.rem(tp, 2)
    z, x = lax.div(ep, 4), lax.rem(ep, 4)
    yp, ym, yo = lax.rem(y + 1, 4), lax.rem(y + 3, 4), lax.rem(y + 2, 4)
    oc = 1 - c
    partner = y * 2 + oc
    up, down = yp * 2 + c, ym * 2 + c
    def send(src, dst, exchange, rs, device):
        pltpu.make_async_remote_copy(
            src_ref=src, dst_ref=dst, send_sem=send_sem.at[exchange], recv_sem=rs, device_id=device, device_id_type=MESH
        ).start()

    def remote(ref, exchange, rs):
        return pltpu.make_async_remote_copy(
            src_ref=ref, dst_ref=ref, send_sem=send_sem.at[exchange], recv_sem=rs, device_id=(ep, partner),
            device_id_type=MESH,
        )

    def arrive(dst, rs):
        remote(dst, 0, rs).wait_recv()

    def left(ref, exchange):
        remote(ref, exchange, g1_r.at[0]).wait_send()

    groups = [
        [(residual, g1.at[tp])],
        [(w_in, v_win)],
        [(mix_gain, v_gain.at[0]), (ffn_gain, v_gain.at[1])],
        [(decay_rate, v_lam.at[0]), (rotation, v_lam.at[1])],
        [(log_step, v_step)],
        [(in_re, v_io.at[0]), (in_im, v_io.at[1]), (read_re, v_io.at[2]), (read_im, v_io.at[3])],
        [(skip, v_skip)],
        [(routes, v_routes)],
        [(weights, v_weights)],
        [(w_glu, v_glu)],
        [(w_out, v_out)],
        [(state, v_state)],
        [(w_gate, v_gu.at[0]), (w_up, v_gu.at[1])],
        [(w_down, v_down)],
    ]
    wholes = [
        g1.at[tp], v_win, v_gain, v_lam, v_step, v_io, v_skip, v_routes, v_weights, v_glu, v_out, v_state, v_gu, v_down
    ]

    def load(i):
        for src, dst in groups[i]:
            pltpu.make_async_copy(src, dst, load_sem.at[i]).start()

    def loaded(i):
        pltpu.make_async_copy(wholes[i], wholes[i], load_sem.at[i]).wait()

    load(0)

    barrier = pltpu.get_barrier_semaphore()
    for d in range(1, NTP):
        pl.semaphore_signal(barrier, inc=1, device_id=(ep, lax.rem(tp + d, NTP)), device_id_type=MESH)
    for d in range(1, NEP):
        pl.semaphore_signal(barrier, inc=1, device_id=(lax.rem(ep + d, NEP), tp), device_id_type=MESH)

    for i in range(1, len(groups)):
        load(i)

    order = (yo, yp, ym, y)

    def columns(t):
        return pl.ds(pl.multiple_of(t * WIDTH, WIDTH), WIDTH)

    def split_send(buf, half, rs, rows):
        first, size = rows
        lo_half, hi_half = (first, half), (first + half, half)
        send(buf(tp, *lo_half), buf(tp, *lo_half), 0, rs(0), (ep, up))
        send(buf(tp, *hi_half), buf(tp, *hi_half), 0, rs(1), (ep, down))
        send(buf(tp, *hi_half), buf(tp, *hi_half), 0, rs(2), (ep, up))
        send(buf(tp, *lo_half), buf(tp, *lo_half), 0, rs(3), (ep, down))
        send(buf(tp, *rows), buf(tp, *rows), 0, rs(4), (ep, partner))

    def split_relay(buf, half, rs, rows):
        first, size = rows
        lo_half, hi_half = (first, half), (first + half, half)
        arrive(buf(down, *lo_half), rs(0))
        send(buf(down, *lo_half), buf(down, *lo_half), 0, rs(5), (ep, up))
        send(buf(down, *lo_half), buf(down, *lo_half), 0, rs(8), (ep, up_oc))
        arrive(buf(up, *hi_half), rs(1))
        send(buf(up, *hi_half), buf(up, *hi_half), 0, rs(5), (ep, down))
        send(buf(up, *hi_half), buf(up, *hi_half), 0, rs(8), (ep, down_oc))
        arrive(buf(down, *hi_half), rs(2))
        send(buf(down, *rows), buf(down, *rows), 0, rs(6), (ep, partner))
        arrive(buf(up, *lo_half), rs(3))
        send(buf(up, *rows), buf(up, *rows), 0, rs(7), (ep, partner))

    far, far_oc = yo * 2 + c, yo * 2 + oc
    up_oc, down_oc = yp * 2 + oc, ym * 2 + oc

    def at1(t, first, size):
        return g1.at[t, pl.ds(first, size), :]

    one = (at1, ROWS // 2, lambda k: g1_r.at[k], (0, ROWS))
    loaded(0)
    pl.semaphore_wait(barrier, NTP + NEP - 2)
    split_send(*one)
    for i in range(3, 9):
        loaded(i)

    eye8 = iota((GRP, GRP), 0) == iota((GRP, GRP), 1)
    step = jnp.exp(jnp.sum(jnp.where(eye8, jnp.broadcast_to(v_step[...], (GRP, GRP)), 0.0), axis=1, keepdims=True))
    rate, rot = v_lam[0], v_lam[1]
    real = -rate
    magnitude = jnp.exp(real * step)
    angle = rot * step
    decay_re = magnitude * jnp.cos(angle)
    decay_im = magnitude * jnp.sin(angle)
    denominator = real * real + rot * rot
    lift_re = ((decay_re - 1.0) * real + decay_im * rot) / denominator
    lift_im = (decay_im * real - (decay_re - 1.0) * rot) / denominator
    bd_hi[...] = jnp.zeros_like(bd_hi)
    bd_lo[...] = jnp.zeros_like(bd_lo)
    rbd[...] = jnp.zeros_like(rbd)
    fresh[...] = jnp.zeros_like(fresh)
    for g in range(GRP):
        rows = slice(g * GCH, (g + 1) * GCH)
        l_re, l_im = lift_re[g:g + 1, :], lift_im[g:g + 1, :]
        b_re, b_im = v_io[0, rows, :], v_io[1, rows, :]
        for n, value in enumerate((l_re * b_re - l_im * b_im, l_re * b_im + l_im * b_re)):
            lanes = slice((2 * g + n) * 128, (2 * g + n) * 128 + STATE)
            hi = value.astype(BF)
            bd_hi[rows, lanes] = hi
            bd_lo[rows, lanes] = (value - hi.astype(F32)).astype(BF)
        rbd[rows, (2 * g) * 128:(2 * g) * 128 + STATE] = v_io[2, rows, :].astype(BF)
        rbd[rows, (2 * g + 1) * 128:(2 * g + 1) * 128 + STATE] = (-v_io[3, rows, :]).astype(BF)
    loaded(11)
    for g in range(GRP):
        old_re = v_state[pl.ds(g, ROWS, stride=2 * GRP), :]
        old_im = v_state[pl.ds(GRP + g, ROWS, stride=2 * GRP), :]
        k_re, k_im = decay_re[g:g + 1, :], decay_im[g:g + 1, :]
        kept_re, kept_im = k_re * old_re - k_im * old_im, k_re * old_im + k_im * old_re
        state_out[pl.ds(g, ROWS, stride=2 * GRP), :] = kept_re
        state_out[pl.ds(GRP + g, ROWS, stride=2 * GRP), :] = kept_im
        fresh[:, (2 * g) * 128:(2 * g) * 128 + STATE] = kept_re.astype(BF)
        fresh[:, (2 * g + 1) * 128:(2 * g + 1) * 128 + STATE] = kept_im.astype(BF)
    act32[...] = dot_nt(fresh[...], rbd[...])
    through = dot_nt(bd_hi[...], rbd[...]) + dot_nt(bd_lo[...], rbd[...])
    through_hi = through.astype(BF)
    thru[0] = through_hi
    thru[1] = (through - through_hi.astype(F32)).astype(BF)
    tiler = (iota((GCH, 128), 0) == lax.rem(iota((GCH, 128), 1), GCH)).astype(BF)
    skip_hi = v_skip[...].astype(BF)
    skip_rest = v_skip[...] - skip_hi.astype(F32)
    skip_mid = skip_rest.astype(BF)
    skip_lo = (skip_rest - skip_mid.astype(F32)).astype(BF)
    skip_rep = dot(skip_hi, tiler) + dot(skip_mid, tiler) + dot(skip_lo, tiler)
    skip_row = jnp.sum(
        jnp.where(lax.div(iota((GRP, 128), 1), GCH) == iota((GRP, 128), 0), skip_rep, 0.0), axis=0, keepdims=True
    )
    r0, r1 = v_routes[0:1, :], v_routes[1:2, :]
    oh0 = (r0 == iota((NEP, ROWS), 0)).astype(F32)
    oh1 = (r1 == iota((NEP, ROWS), 0)).astype(F32)
    upper_tri = (iota((ROWS, ROWS), 0) < iota((ROWS, ROWS), 1)).astype(BF)
    before = dot((oh0 + oh1).astype(BF), upper_tri)
    dest0 = r0.astype(F32) * SLOT + jnp.sum(before * oh0, axis=0, keepdims=True)
    dest1 = r1.astype(F32) * SLOT + jnp.sum(before * oh1, axis=0, keepdims=True)
    place = iota((SLOTS, ROWS), 0).astype(F32)
    m0, m1 = (dest0 == place).astype(F32), (dest1 == place).astype(F32)
    d_map[...] = (m0 + m1).astype(BF)
    w_all = jnp.transpose(v_weights[0:1, :] * m0 + v_weights[1:2, :] * m1)
    w_hi = w_all.astype(BF)
    wt[0] = w_hi
    wt[1] = (w_all - w_hi.astype(F32)).astype(BF)

    loaded(1)
    loaded(2)
    loaded(9)
    loaded(10)
    send(v_glu, v_glu2, 1, d_r.at[0], (ep, partner))
    for j in range(4):
        send(v_out.at[:, columns(order[j] * 2 + oc)], wo2.at[j], 2, d_r.at[1], (ep, partner))

    total = [None, None]

    def mix_block(t):
        rows = g1[t].astype(F32)
        squares = jnp.sum(rows * rows, axis=1, keepdims=True)
        gain = v_gain[0, :, columns(t)]
        product = dot((rows * gain).astype(BF), v_win[columns(t), :])
        total[0] = squares if total[0] is None else total[0] + squares
        total[1] = product if total[1] is None else total[1] + product

    mix_block(tp)
    split_relay(*one)
    mix_block(down)
    mix_block(up)
    arrive(g1.at[partner], g1_r.at[4])
    mix_block(partner)
    arrive(g1.at[down_oc], g1_r.at[6])
    mix_block(down_oc)
    arrive(g1.at[up_oc], g1_r.at[7])
    mix_block(up_oc)
    arrive(g1.at[far], g1_r.at[5])
    mix_block(far)
    arrive(g1.at[far_oc], g1_r.at[8])
    mix_block(far_oc)
    u_in = (total[1] * lax.rsqrt(total[0] / (NTP * WIDTH) + EPS)).astype(BF)

    act = jax.nn.gelu(act32[...] + dot(u_in, thru[0]) + dot(u_in, thru[1]) + skip_row * u_in.astype(F32))
    act32[...] = act
    act_all[tp] = act.astype(BF)
    towards = (far, far_oc, up, down, up_oc, down_oc, partner)
    for t in towards:
        send(act_all.at[tp], act_all.at[tp], 3, a_r.at[0], (ep, t))
    drive = dot(u_in, bd_hi[...]) + dot(u_in, bd_lo[...])
    for g in range(GRP):
        state_out[pl.ds(g, ROWS, stride=2 * GRP), :] += drive[:, (2 * g) * 128:(2 * g) * 128 + STATE]
        state_out[pl.ds(GRP + g, ROWS, stride=2 * GRP), :] += drive[:, (2 * g + 1) * 128:(2 * g + 1) * 128 + STATE]
    arrive(v_glu2, d_r.at[0])
    arrive(wo2, d_r.at[1])
    arrive(act_all.at[0:NTP - 1], a_r.at[0])
    everything = jnp.concatenate([act_all[t] for t in range(NTP)], axis=1)
    mixed[0] = (act32[...] * jax.nn.sigmoid(dot(everything, v_glu[...]))).astype(BF)
    mixed[1] = (act_all[partner].astype(F32) * jax.nn.sigmoid(dot(everything, v_glu2[...]))).astype(BF)

    def scatter(q, rel, dire, mrg, ms, exchange, rs, base, piece, lo, hi):
        low, high = pl.ds(lo, piece), pl.ds(hi, piece)

        def far_blocks():
            send(q.at[0, low, :], rel.at[0], exchange, rs.at[base], (ep, up))
            send(q.at[0, high, :], rel.at[1], exchange, rs.at[base + 1], (ep, down))

        def near_up():
            send(q.at[1, high, :], dire.at[0], exchange, rs.at[base + 2], (ep, up))

        def near_down():
            send(q.at[2, low, :], dire.at[1], exchange, rs.at[base + 3], (ep, down))

        def merge():
            arrive(rel.at[0], rs.at[base])
            ms[0] = (q[1, lo:lo + piece, :].astype(F32) + rel[0].astype(F32)).astype(BF)
            send(ms.at[0], mrg.at[0], exchange, rs.at[base + 4], (ep, up))
            arrive(rel.at[1], rs.at[base + 1])
            ms[1] = (q[2, hi:hi + piece, :].astype(F32) + rel[1].astype(F32)).astype(BF)
            send(ms.at[1], mrg.at[1], exchange, rs.at[base + 5], (ep, down))

        def final(own, done):
            arrive(dire.at[1], rs.at[base + 3])
            arrive(mrg.at[0], rs.at[base + 4])
            done(0, own[lo:lo + piece, :] + dire[1].astype(F32) + mrg[0].astype(F32))
            arrive(dire.at[0], rs.at[base + 2])
            arrive(mrg.at[1], rs.at[base + 5])
            done(1, own[hi:hi + piece, :] + dire[0].astype(F32) + mrg[1].astype(F32))

        return far_blocks, near_up, near_down, merge, final

    def branch_done(part, value):
        rows = slice(part * (ROWS // 2), (part + 1) * (ROWS // 2))
        after[rows, :] = (g1[tp, rows, :].astype(F32) + value).astype(BF)

    def chip_product(j):
        return dot(mixed[0], v_out[:, columns(order[j] * 2 + c)]) + dot(mixed[1], wo2[j])

    far_blocks, near_up, near_down, merge, final = scatter(
        b_q, b_rel, b_dir, b_mrg, b_ms, 4, b_r, 0, ROWS // 2, 0, ROWS // 2
    )
    b_q[0] = chip_product(0).astype(BF)
    far_blocks()
    b_q[1] = chip_product(1).astype(BF)
    near_up()
    b_q[2] = chip_product(2).astype(BF)
    near_down()
    b_own[...] = chip_product(3)
    merge()
    final(b_own, branch_done)

    outb[...] = dot(d_map[...], after[...]).astype(BF)

    def slot(e):
        return pl.ds(pl.multiple_of(e * SLOT, SLOT), SLOT)

    chunk = SLOTS // 4
    turns = (
        ((2, 2), (2, 1), (2, 3), (3, 2)), ((1, 2), (3, 3), (3, 1), (1, 3)),
        ((1, 1), (2, 0), (0, 2), (3, 0)), ((1, 0), (0, 3), (0, 1), (0, 0)),
    )

    def rows_of(j):
        return pl.ds(j * chunk, chunk)

    for j in (3, 2, 1, 0):
        for m, (dz, dx) in enumerate(turns[j]):
            here = slice(j * chunk + m * SLOT, j * chunk + (m + 1) * SLOT)
            if dz or dx:
                e = lax.rem(z + dz, 4) * 4 + lax.rem(x + dx, 4)
                send(outb.at[slot(e), :], g2.at[tp, here, :], 5, x_r.at[j], (e, tp))
            else:
                g2[tp, here, :] = outb[slot(ep), :]
    loaded(12)

    def start_chunk(j):
        arrive(g2.at[tp, pl.ds(j * chunk, chunk if j < 3 else chunk - SLOT), :], x_r.at[j])
        block = g2.at[tp, rows_of(j), :]
        send(block, block, 6, g2_r.at[j], (ep, up))
        send(block, block, 6, g2_r.at[4 + j], (ep, down))
        send(block, block, 6, g2_r.at[12], (ep, partner))

    def relay(j):
        first = g2.at[down, rows_of(j), :]
        arrive(first, g2_r.at[j])
        low = g2.at[down, pl.ds(j * chunk, chunk // 2), :]
        send(low, low, 6, g2_r.at[8 + j], (ep, up))
        send(first, first, 6, g2_r.at[13], (ep, partner))
        second = g2.at[up, rows_of(j), :]
        arrive(second, g2_r.at[4 + j])
        high = g2.at[up, pl.ds(j * chunk + chunk // 2, chunk // 2), :]
        send(high, high, 6, g2_r.at[8 + j], (ep, down))
        send(second, second, 6, g2_r.at[14], (ep, partner))

    def pass_far(j):
        block = g2.at[far, rows_of(j), :]
        arrive(block, g2_r.at[8 + j])
        send(block, block, 6, g2_r.at[15], (ep, partner))

    def expert_block(t, first=False):
        rows = g2[t].astype(F32)
        scaled = (rows * v_gain[1, :, columns(t)]).astype(BF)
        squares = rows * rows
        squares = squares[:, 0:128] + squares[:, 128:256] + squares[:, 256:384] + squares[:, 384:512]
        gate, upper = dot_nt(scaled, v_gu[0, :, columns(t)]), dot_nt(scaled, v_gu[1, :, columns(t)])
        if first:
            sq[...] = squares
            acc_g[...] = gate
            acc_u[...] = upper
        else:
            sq[...] += squares
            acc_g[...] += gate
            acc_u[...] += upper

    def from_partner(t, k):
        arrive(g2.at[t], g2_r.at[k])
        expert_block(t)

    for j in (3, 2, 1, 0):
        start_chunk(j)
    expert_block(tp, True)
    relay(3)
    relay(2)
    from_partner(partner, 12)
    relay(1)
    relay(0)
    expert_block(down)
    pass_far(3)
    expert_block(up)
    pass_far(2)
    from_partner(down_oc, 13)
    pass_far(1)
    from_partner(up_oc, 14)
    pass_far(0)
    expert_block(far)
    from_partner(far_oc, 15)

    def activate(i):
        for r in (2 * i * chunk, (2 * i + 1) * chunk):
            scale = lax.rsqrt(jnp.sum(sq[r:r + 64, :], axis=1, keepdims=True) / (NTP * WIDTH) + EPS)
            gate, upper = acc_g[r:r + 64, :] * scale, acc_u[r:r + 64, :] * scale
            hidden[r:r + 64, :] = (gate * jax.nn.sigmoid(gate) * upper).astype(BF)

    def far_partner(i):
        rows = slice(2 * i * chunk, 2 * (i + 1) * chunk)
        e_ds[0, rows, :] = dot(hidden[rows, :], v_down[:, columns(far_oc)]).astype(BF)
        send(e_ds.at[0, rows, :], e_dr.at[0, rows, :], 7, e_r.at[16 * i], (ep, partner))

    def far_chip(i):
        rows = slice(2 * i * chunk, 2 * (i + 1) * chunk)
        value = dot(hidden[rows, :], v_down[:, columns(far)])
        arrive(e_dr.at[0, rows, :], e_r.at[16 * i])
        e_q[0, rows, :] = (value + e_dr[0, rows, :].astype(F32)).astype(BF)

    def product(t):
        return dot(hidden[...], v_down[:, columns(t)])

    def to_partner(j):
        e_ds[j] = product(order[j] * 2 + oc).astype(BF)
        send(e_ds.at[j], e_dr.at[j], 7, e_r.at[j], (ep, partner))

    def on_chip(j):
        value = product(order[j] * 2 + c)
        arrive(e_dr.at[j], e_r.at[j])
        return value + e_dr[j].astype(F32)

    def expert_done(i):
        def done(part, value):
            j = 2 * i + part
            eout[j * chunk:(j + 1) * chunk, :] = value.astype(BF)
            for m, (dz, dx) in enumerate(turns[j]):
                here = slice(j * chunk + m * SLOT, j * chunk + (m + 1) * SLOT)
                if dz or dx:
                    s = lax.rem(z + 4 - dz, 4) * 4 + lax.rem(x + 4 - dx, 4)
                    send(eout.at[here, :], back.at[slot(ep), :], 9, ret_r.at[0], (s, tp))
                else:
                    back[slot(ep), :] = eout[here, :]
        return done

    stages = [
        scatter(
            e_q, e_rel.at[i], e_dir.at[i], e_mrg.at[i], e_ms.at[i], 8, e_r, 4 + 6 * i, chunk, 2 * i * chunk, (2 * i + 1) * chunk
        )
        for i in range(2)
    ]
    activate(0)
    loaded(13)
    far_partner(0)
    activate(1)
    far_partner(1)
    to_partner(1)
    far_chip(0)
    stages[0][0]()
    far_chip(1)
    stages[1][0]()
    to_partner(2)
    to_partner(3)
    e_q[1] = on_chip(1).astype(BF)
    stages[0][1]()
    e_q[2] = on_chip(2).astype(BF)
    stages[0][2]()
    e_own[...] = on_chip(3)
    stages[0][3]()
    stages[1][1]()
    stages[1][2]()
    stages[1][3]()
    stages[0][4](e_own, expert_done(0))
    stages[1][4](e_own, expert_done(1))
    arrive(back.at[0:SLOTS - SLOT, :], ret_r.at[0])
    combined = dot(wt[0], back[...]) + dot(wt[1], back[...])
    out[...] = (after[...].astype(F32) + combined).astype(BF)
    left(g1.at[0:NTP - 1], 0)
    left(v_glu, 1)
    left(wo2, 2)
    left(act_all.at[0:NTP - 1], 3)
    left(b_q, 4)
    left(outb.at[0:SLOTS - SLOT, :], 5)
    left(g2.at[0:NTP - 1], 6)
    left(e_ds, 7)
    left(e_q, 8)
    left(eout.at[0:SLOTS - SLOT, :], 9)


def write_out(layer, state, layer_hbm, state_hbm, sems):
    copies = [pltpu.make_async_copy(state, state_hbm, sems.at[0]), pltpu.make_async_copy(layer, layer_hbm, sems.at[1])]
    for copy in copies:
        copy.start()
    for copy in copies:
        copy.wait()


def per_device(
    residual, routes, route_weights, state_prev, mix_gain, ffn_gain, w_in, decay_rate, rotation,
    log_step, in_re, in_im, read_re, read_im, skip_gain, w_glu, w_out, w_gate, w_up, w_down,
):
    dma = pltpu.SemaphoreType.DMA
    vm = pltpu.VMEM
    operands = (
        residual, routes.T, route_weights.T, state_prev.reshape(ROWS * 2 * GRP, STATE), mix_gain.reshape(1, -1),
        ffn_gain.reshape(1, -1), w_in, decay_rate, rotation, log_step.reshape(1, GRP),
        in_re.transpose(0, 2, 1).reshape(GRP * GCH, STATE), in_im.transpose(0, 2, 1).reshape(GRP * GCH, STATE), read_re.reshape(GRP * GCH, STATE),
        read_im.reshape(GRP * GCH, STATE), skip_gain, w_glu, w_out, w_gate[0].T, w_up[0].T, w_down[0],
    )

    def exchange(lead, rows, part):
        return [vm((3, rows, WIDTH), BF), vm((rows, WIDTH), F32)] + [vm((*lead, 2, part, WIDTH), BF)] * 4

    scratch = [
        vm((2, ROWS), jnp.int32), vm((2, ROWS), F32), vm((ROWS * 2 * GRP, STATE), F32), vm((2, 1, NTP * WIDTH), F32),
        vm((NTP * WIDTH, 128), BF), vm((2, GRP, STATE), F32), vm((1, GRP), F32), vm((4, GRP * GCH, STATE), F32),
        vm((GRP, GCH), F32), vm((NEP * ROWS, 128), BF), vm((128, NTP * WIDTH), BF), vm((2, FFW, NTP * WIDTH), BF),
        vm((FFW, NTP * WIDTH), BF),
    ]
    scratch += [
        vm((NTP, ROWS, WIDTH), BF), vm((2, 128, 128), BF), vm((128, 2048), BF), vm((128, 2048), BF),
        vm((128, 2048), BF), vm((ROWS, 2048), BF), vm((NTP, ROWS, 128), BF),
        vm((ROWS, 128), F32), vm((2, ROWS, 128), BF),
    ]
    scratch += exchange((), ROWS, ROWS // 2)
    scratch += [
        vm((NEP * ROWS, 128), BF), vm((4, 128, WIDTH), BF),
        vm((ROWS, WIDTH), BF), vm((SLOTS, ROWS), BF), vm((2, ROWS, SLOTS), BF), vm((SLOTS, WIDTH), BF),
        vm((NTP, SLOTS, WIDTH), BF), vm((SLOTS, FFW), F32), vm((SLOTS, FFW), F32), vm((SLOTS, 128), F32),
        vm((SLOTS, FFW), BF),
    ]
    scratch += [vm((4, SLOTS, WIDTH), BF)] * 2 + exchange((2,), SLOTS, SLOTS // 4)
    scratch += [vm((SLOTS, WIDTH), BF), vm((SLOTS, WIDTH), BF)]
    scratch += [
        dma((14,)), dma((10,)), dma((9,)), dma((1,)), dma((6,)), dma((2,)), dma((4,)), dma((16,)), dma((17,)), dma((1,))
    ]
    anywhere = pl.BlockSpec(memory_space=pltpu.HBM)
    outside = pl.BlockSpec(memory_space=pl.ANY)
    inside = pl.BlockSpec(memory_space=pltpu.VMEM)
    layer_out, state_next = pl.pallas_call(
        kernel,
        out_shape=(vm((ROWS, WIDTH), BF), vm((ROWS * 2 * GRP, STATE), F32)),
        in_specs=[anywhere] * 20,
        out_specs=(inside, inside),
        scratch_shapes=scratch,
        compiler_params=pltpu.CompilerParams(
            collective_id=0, has_side_effects=True, vmem_limit_bytes=44 * 1024 * 1024
        ),
        name="layer",
    )(*[pltpu.with_memory_space_constraint(a, pltpu.HBM) for a in operands])
    layer_out = pltpu.with_memory_space_constraint(layer_out, pltpu.VMEM)
    state_next = pltpu.with_memory_space_constraint(state_next, pltpu.VMEM)
    layer_out, state_next = pl.pallas_call(
        write_out,
        out_shape=(
            jax.ShapeDtypeStruct((ROWS, WIDTH), BF),
            jax.ShapeDtypeStruct((ROWS * 2 * GRP, STATE), F32),
        ),
        in_specs=[inside] * 2,
        out_specs=(outside, outside),
        scratch_shapes=[dma((2,))],
        name="write_out",
    )(layer_out, state_next)
    return layer_out, state_next.reshape(ROWS, 2, GRP, STATE)


def solution(mesh):
    return jax.shard_map(
        per_device,
        mesh=mesh,
        in_specs=(
            P("ep", "tp"), P("ep", None), P("ep", None), P("ep", None, "tp", None), P(), P(), P(None, "tp"),
            P("tp", None), P("tp", None), P("tp"), P("tp", None, None), P("tp", None, None), P("tp", None, None),
            P("tp", None, None), P("tp", None), P(None, "tp"), P("tp", None), P("ep", None, "tp"),
            P("ep", None, "tp"), P("ep", "tp", None),
        ),
        out_specs=(P("ep", "tp"), P("ep", None, "tp", None)),
        check_vma=False,
    )
```
